512 devices in a mesh: fs: 64 (over z, y), tp: 8 (over x, core).
Axes of the slice: x: 4, y: 8, z: 8, core: 2. Of those that a mesh axis runs over, the one named last changes fastest.
Arguments:
- prompt: bfloat16 [8192, 2048], P('fs'), may hold values from -6 to 6
- norm_gain: float32 [2048], P('fs'), may hold values from 0.1 to 1.9
- gate_train: float32 [2048, 32768], P('fs', 'tp'), may hold values from -0.125 to 0.125
- up_train: float32 [2048, 32768], P('fs', 'tp'), may hold values from -0.125 to 0.125
- down_train: float32 [2048, 32768], P('fs', 'tp'), may hold values from -0.25 to 0.25
- common_gate_train: float32 [2048, 512], P('fs', 'tp'), may hold values from -0.125 to 0.125
- common_up_train: float32 [2048, 512], P('fs', 'tp'), may hold values from -0.125 to 0.125
- common_down_train: float32 [2048, 512], P('fs', 'tp'), may hold values from -0.25 to 0.25
- route_ids: int32 [8192, 6], P('fs'), may hold values from 0 to 63, all different within a row; in each aligned block of 128 rows (0 to 127, 128 to 255, ...) at most 16 rows name the same one
- route_weights: float32 [8192, 6], P('fs'), may hold values from 0.1 to 1
Outputs:
- mixture: bfloat16 [8192, 2048], P('fs', 'tp')
- gate_serve: bfloat16 [64, 512, 2048], P('fs', 'tp')
- up_serve: bfloat16 [64, 512, 2048], P('fs', 'tp')
- down_serve: bfloat16 [64, 512, 2048], P('fs', 'tp')
- common_gate_serve: bfloat16 [512, 2048], P('tp')
- common_up_serve: bfloat16 [512, 2048], P('tp')
- common_down_serve: bfloat16 [512, 2048], P('tp')
The draws below stay inside these ranges and needn't reach their ends.
Inputs may be any that keep to these rules, and one draw needn't show every extreme that they name: `route_ids`: each row names 6 different experts. Among the rows of one index of fs no expert is named more than 16 times, and in every draw some expert is named exactly 16 times by the rows of some index.
All inputs are finite; a program needn't handle non-finite values.
Results may differ from the reference program's by a relative error of at most 0.011.
Values may be sent and summed in bfloat16 or wider, within the bound.
No kernel may reach another device: no remote copies, remote signals or barrier semaphores. Data moves between devices by JAX's collectives and lax.ppermute only.
A program may use at most 64 MiB of HBM per device.

```python
import math
import jax
import jax.numpy as jnp
import numpy as np
from jax import lax

D = 2048
FF = 512
SFF = 512
E = 64
TOP_K = 6
TOK_DEV = 128
CAP = 16
TOKENS = 8192
N_FS = 64
N_TP = 8


def shard_levels(key, extent, pieces, smallest, top_value):
    def one(dim, parts):
        draws = jax.random.uniform(jax.random.fold_in(jax.random.fold_in(key, 6), dim), (parts,), jnp.float32, smallest / len(pieces), top_value / len(pieces))
        return jnp.repeat(jnp.exp(draws), extent[dim] // parts).reshape((-1,) + (1,) * (len(extent) - dim - 1))

    factor_of = one(*pieces[0])
    for cut in pieces[1:]:
        factor_of = factor_of * one(*cut)
    return factor_of


def deal_out(rng, own, number, rows, amount, top, bound, lean):
    order = jax.random.permutation(rng, amount)
    packed, usual = portions_of(amount, rows * top, bound, lean, True), portions_of(amount, rows * top, bound, lean, False)
    places = jnp.arange(amount)

    def named(lengths, rotation):
        used = int((lengths > 0).sum())
        fixed = max(1, used // 4)
        passed = fixed + (places - fixed + rotation * (used - fixed)) % max(1, amount - fixed)
        return jnp.zeros((amount,), jnp.int32).at[order[jnp.where(places < fixed, places, passed)]].set(jnp.asarray(lengths, jnp.int32))

    lengths = jnp.where(number % 4 == 0, named(packed, number // 4), named(usual, number - number // 4 - 1))
    mixed = jax.random.permutation(jax.random.fold_in(own, 3), amount)
    giver, receiver = mixed[0:amount // 2 * 2:2], mixed[1:amount // 2 * 2:2]
    room = jnp.minimum(lengths[giver] - 1, bound - lengths[receiver]) // 2
    room = jnp.where((giver == order[0]) | (receiver == order[0]) | (lengths[receiver] == 0), 0, jnp.maximum(room, 0))
    passed = jax.random.randint(jax.random.fold_in(own, 4), (amount // 2,), 0, 1 << 20) % (room + 1)
    lengths = lengths.at[giver].add(-passed).at[receiver].add(passed)
    items = jnp.searchsorted(jnp.cumsum(lengths), jnp.arange(rows * top), side="right").astype(jnp.int32)
    listing = items.reshape(top, rows).T
    listing = listing[jax.random.permutation(jax.random.fold_in(own, 1), rows)]
    rotation = jax.random.randint(jax.random.fold_in(own, 2), (rows, 1), 0, top)
    return jnp.take_along_axis(listing, (jnp.arange(top)[None, :] + rotation) % top, axis=1)


def portions_of(amount, total, limit, skew, full):
    portions = [(1 << 20) // math.isqrt(rank ** skew) + 1 for rank in range(1, amount + 1)]
    largest = limit if full else min(limit, max(-(-total // amount), total * portions[0] // sum(portions)))
    least = 1 if total - largest >= amount - 1 else 0
    counts, rest = [largest] + [least] * (amount - 1), total - largest - least * (amount - 1)
    while rest > 0:
        free = [i for i in range(1, amount) if counts[i] < largest] or [i for i in range(1, amount) if counts[i] < limit]
        pool, budget = sum([portions[i] for i in free]), rest
        for i in free:
            extra = min(limit - counts[i], max(1, budget * portions[i] // pool), rest)
            counts[i] = counts[i] + extra
            rest = rest - extra
    return np.array(counts)


def centred(key, shape, deviation, limit, shards=(), kind=jnp.bfloat16):
    array = deviation * jax.random.normal(key, shape, jnp.float32)
    if shards:
        array = array * shard_levels(key, shape, shards, -0.22, 0.18)
    return jnp.clip(array, -limit, limit).astype(kind)


def setup_inputs(seed: int = 0) -> dict:
    key_list = jax.random.split(jax.random.key(seed), 11)
    prompt = centred(key_list[0], (TOKENS, D), 1.0, 6.0, ((0, 64),))
    norm_gain = jnp.clip(1.0 + 0.18 * jax.random.normal(key_list[1], (D,), jnp.float32), 0.1, 1.9)
    gate_train = centred(key_list[2], (D, E * FF), D ** -0.5, 0.125, ((0, 64), (1, 8)), jnp.float32)
    up_train = centred(key_list[3], (D, E * FF), D ** -0.5, 0.125, ((0, 64), (1, 8)), jnp.float32)
    down_train = centred(key_list[4], (D, E * FF), FF ** -0.5, 0.25, ((0, 64), (1, 8)), jnp.float32)
    common_gate_train = centred(key_list[5], (D, SFF), D ** -0.5, 0.125, ((0, 64), (1, 8)), jnp.float32)
    common_up_train = centred(key_list[6], (D, SFF), D ** -0.5, 0.125, ((0, 64), (1, 8)), jnp.float32)
    common_down_train = centred(key_list[7], (D, SFF), SFF ** -0.5, 0.25, ((0, 64), (1, 8)), jnp.float32)
    route_ids_keys = jax.random.split(jax.random.fold_in(key_list[8], 1), TOKENS // TOK_DEV)
    route_ids_turns = jax.random.permutation(jax.random.fold_in(key_list[8], 3), TOKENS // TOK_DEV)
    route_ids = jax.vmap(lambda own, number: deal_out(jax.random.fold_in(key_list[8], 2), own, number, TOK_DEV, E, TOP_K, CAP, 2))(route_ids_keys, route_ids_turns).reshape((TOKENS, TOP_K))
    route_weights = jnp.clip(jnp.exp(math.log(1.0) - 2.3025851 * jax.random.uniform(key_list[9], (TOKENS, TOP_K), jnp.float32) ** shard_levels(key_list[9], (TOKENS, TOP_K), ((0, 64),), -0.2, 0.2)), 0.1, 1.0)
    return {"prompt": prompt, "norm_gain": norm_gain, "gate_train": gate_train, "up_train": up_train, "down_train": down_train, "common_gate_train": common_gate_train, "common_up_train": common_up_train, "common_down_train": common_down_train, "route_ids": route_ids, "route_weights": route_weights}


epsilon = 1e-06

def slot_table(route_ids):
    groups = route_ids.reshape(N_FS, TOK_DEV * TOP_K)
    onehot = (groups[:, :, None] == jnp.arange(E, dtype=jnp.int32)[None, None, :]).astype(jnp.int32)
    before = jnp.cumsum(onehot, axis=1) - onehot
    slot_of = lax.optimization_barrier(jnp.sum(before * onehot, axis=2)).astype(jnp.int32)
    source = jnp.arange(N_FS, dtype=jnp.int32)[:, None]
    return (groups * (N_FS * CAP) + source * CAP + slot_of).reshape(-1).astype(jnp.int32)

def rounded_sum(hidden, down_matrix):
    span = hidden.shape[1] // N_TP
    running = jnp.zeros((hidden.shape[0], down_matrix.shape[1]), jnp.float32)
    for member in range(N_TP):
        partial_value = jnp.dot(hidden[:, member * span:(member + 1) * span], down_matrix[member * span:(member + 1) * span], preferred_element_type=jnp.float32).astype(jnp.bfloat16)
        running = running + lax.optimization_barrier(partial_value).astype(jnp.float32)
    return running.astype(jnp.bfloat16)

def to_serve(matrix):
    return jnp.transpose(matrix.reshape(D, E, FF), (1, 2, 0)).astype(jnp.bfloat16)

def reference(prompt, norm_gain, gate_train, up_train, down_train, common_gate_train, common_up_train, common_down_train, route_ids, route_weights):
    gain_col = norm_gain[:, None]
    gate_serve = to_serve(gate_train * gain_col)
    up_serve = to_serve(up_train * gain_col)
    down_serve = to_serve(down_train)
    common_gate_serve = jnp.transpose(common_gate_train * gain_col).astype(jnp.bfloat16)
    common_up_serve = jnp.transpose(common_up_train * gain_col).astype(jnp.bfloat16)
    common_down_serve = jnp.transpose(common_down_train).astype(jnp.bfloat16)
    values = prompt.astype(jnp.float32)
    normed = (values * lax.rsqrt(lax.optimization_barrier(jnp.mean(values * values, axis=1, keepdims=True)) + epsilon)).astype(jnp.bfloat16)
    target = slot_table(route_ids)
    pair_rows = jnp.repeat(normed, TOP_K, axis=0)
    buffer = jnp.zeros((E * N_FS * CAP, D), jnp.bfloat16).at[target].set(pair_rows).reshape(E, N_FS * CAP, D)

    def expert(operands):
        slot_rows, gate_matrix, up_matrix, down_matrix = operands
        gate_value = jnp.dot(slot_rows, gate_matrix.T, preferred_element_type=jnp.float32)
        up_value = jnp.dot(slot_rows, up_matrix.T, preferred_element_type=jnp.float32)
        hidden = (jax.nn.silu(gate_value) * up_value).astype(jnp.bfloat16)
        return rounded_sum(hidden, down_matrix)
    outputs = lax.map(expert, (buffer, gate_serve, up_serve, down_serve))
    picked = outputs.reshape(E * N_FS * CAP, D)[target].astype(jnp.float32)
    weighted = lax.optimization_barrier(jnp.sum(picked.reshape(TOKENS, TOP_K, D) * route_weights[:, :, None], axis=1))
    common_gate = jnp.dot(normed, common_gate_serve.T, preferred_element_type=jnp.float32)
    common_up = jnp.dot(normed, common_up_serve.T, preferred_element_type=jnp.float32)
    common_hidden = (jax.nn.silu(common_gate) * common_up).astype(jnp.bfloat16)
    common_out = rounded_sum(common_hidden, common_down_serve)
    mixture = (weighted + common_out.astype(jnp.float32)).astype(jnp.bfloat16)
    return (mixture, gate_serve, up_serve, down_serve, common_gate_serve, common_up_serve, common_down_serve)
```

```python
import jax
import jax.numpy as jnp
from jax import lax
from jax.experimental import pallas as pl
from jax.experimental.pallas import tpu as pltpu
from jax.sharding import PartitionSpec as P


E = 64
CAP = 16
TOP_K = 6
TOK = 128
D = 2048
N_FS = 64
N_TP = 8
U = 64
W32 = D // N_FS
COLS = D // N_TP
ROWS = E * CAP
LANES = 128
epsilon = 1e-06

f32 = jnp.float32
bf16 = jnp.bfloat16
VM = pl.BlockSpec(memory_space=pltpu.VMEM)
SM = pl.BlockSpec(memory_space=pltpu.SMEM)


def iota(shape, dim):
    return lax.broadcasted_iota(jnp.int32, shape, dim)


def half_roll(x):
    return pltpu.roll(x, 64, 1)


def call(body, outs, n_in, smem=0, scratch=(), far=(), keep=True):
    flat, tree = jax.tree.flatten(outs)
    kept = [pltpu.VMEM(o.shape, o.dtype) if keep is True or i in keep else o for i, o in enumerate(flat)]
    fn = pl.pallas_call(
        body,
        out_shape=jax.tree.unflatten(tree, kept),
        in_specs=[SM] * smem + [VM] * (n_in - smem),
        out_specs=jax.tree.map(lambda _: VM, outs),
        scratch_shapes=list(scratch),
        compiler_params=pltpu.CompilerParams(vmem_limit_bytes=16 * 2**20),
    )

    def run(*args):
        placed = [
            a if i < smem or i in far else pltpu.with_memory_space_constraint(a, pltpu.VMEM)
            for i, a in enumerate(args)
        ]
        return fn(*placed)

    return run


def dot(a, b):
    return jnp.dot(a, b, preferred_element_type=f32)


def dot_nt(a, b):
    return lax.dot_general(a, b, (((1,), (1,)), ((), ())), preferred_element_type=f32)


def gain_column(gain_ref):
    n = gain_ref.shape[1]
    eye = iota((n, n), 0) == iota((n, n), 1)
    spread = jnp.where(eye, jnp.broadcast_to(gain_ref[...], (n, n)), 0.0)
    return jnp.sum(spread, axis=1, keepdims=True)


def dispatch_body(m_ref, prompt_ref, ids_ref, gain_ref, cg_ref, cu_ref, cd_ref, send_ref, normed_ref, pos_ref):
    m = m_ref[0]
    values = prompt_ref[...].astype(f32)
    scale = lax.rsqrt(jnp.mean(values * values, axis=1, keepdims=True) + epsilon)
    normed_ref[...] = (values * scale).astype(bf16)
    experts = iota((E, TOK), 0)
    named = jnp.zeros((E, TOK), f32)
    for k in range(TOP_K):
        named = jnp.where(ids_ref[k : k + 1, :] == experts, 1.0, named)
    earlier = jnp.where(iota((TOK, TOK), 0) < iota((TOK, TOK), 1), 1.0, 0.0).astype(bf16)
    slot = dot(named.astype(bf16), earlier)
    pos = jnp.where(named > 0.0, slot, -1.0)
    pos_ref[...] = pos
    expand = jnp.where((iota((ROWS, E), 0) >> 4) == iota((ROWS, E), 1), 1.0, 0.0).astype(bf16)
    at = dot(expand, pos.astype(bf16))
    pick = jnp.where(at == (iota((ROWS, TOK), 0) & 15).astype(f32), 1.0, 0.0).astype(bf16)
    mine = normed_ref[:, pl.ds(pl.multiple_of(m * COLS, COLS), COLS)]
    rows = dot(pick, mine).astype(bf16)
    send_ref[:, 0:16, :] = rows[:, :LANES].reshape(E, CAP, LANES)
    send_ref[:, 16:32, :] = rows[:, LANES:].reshape(E, CAP, LANES)
    gain = gain_column(gain_ref)
    both = jnp.concatenate([cg_ref[...] * gain, cu_ref[...] * gain], axis=1)
    down = jnp.concatenate([cd_ref[0:16, :], cd_ref[16:32, :]], axis=1)
    piece = jnp.concatenate([both, down], axis=0).astype(bf16)
    send_ref[:, 32:80, :] = jnp.broadcast_to(piece[None], (N_FS, 48, LANES))


def prepare_body(m_ref, gain_ref, g_ref, u_ref, d_ref, *out_refs):
    m = m_ref[0]
    gain = gain_column(gain_ref)
    low = iota((W32, LANES), 1) < 64
    low16 = iota((16, LANES), 1) < 64
    for k in range(N_TP):
        to = m ^ k
        odd = (to & 1) == 1
        for j in range(8):
            at = pl.ds(pl.multiple_of(j * 512 + (to >> 1) * LANES, LANES), LANES)
            g = g_ref[:, at] * gain
            u = u_ref[:, at] * gain
            d = d_ref[:, at]
            g = jnp.where(odd, half_roll(g), g)
            u = jnp.where(odd, u, half_roll(u))
            out_refs[k][j, 0:32, :] = jnp.where(low, g, u).astype(bf16)
            d0, d1 = d[0:16, :], d[16:32, :]
            d0 = jnp.where(odd, half_roll(d0), d0)
            d1 = jnp.where(odd, d1, half_roll(d1))
            out_refs[k][j, 32:48, :] = jnp.where(low16, d0, d1).astype(bf16)


def assemble_body(m_ref, *refs):
    m = m_ref[0]
    out_ref = refs[-1]
    for k in range(N_TP):
        out_ref[pl.ds(pl.multiple_of((m ^ k) * 8, 8), 8)] = refs[k][...]


def silu(v):
    return v / (1.0 + jnp.exp(-v))


def packed_hidden(acc):
    half = acc.shape[0] // 2
    top, bottom = acc[:half], acc[half:]
    first = silu(top) * half_roll(top)
    second = silu(half_roll(bottom)) * bottom
    return jnp.where(iota((half, LANES), 1) < 64, first, second).astype(bf16)


def common_hidden_body(normed_ref, got_ref, out_ref):
    weights = got_ref[:, 32:64, :].reshape(D, LANES)
    out_ref[...] = packed_hidden(dot(normed_ref[...], weights))


def hidden_body(m_ref, own_ref, left_ref, right_ref, far_a_ref, far_b_ref, three_ref, far_ref, w_ref, common_ref, out_ref, acc_ref):
    m = m_ref[0]

    def joined(x):
        n = x.shape[0]
        return jnp.concatenate([x[:, 0:16, :].reshape(n * 16, LANES), x[:, 16:32, :].reshape(n * 16, LANES)], axis=1)

    def weights(q):
        return w_ref[pl.ds(pl.multiple_of((q & 7) * 8, 8), 8), 0:32, :].reshape(COLS, LANES)

    acc_ref[...] = dot(joined(own_ref[...]), weights(m))
    acc_ref[...] += dot(joined(left_ref[...]), weights(m - 2))
    acc_ref[...] += dot(joined(right_ref[...]), weights(m + 2))
    across = weights(m + 4)
    acc_ref[0:512, :] += dot(joined(far_a_ref[...]), across)
    acc_ref[512:1024, :] += dot(joined(far_b_ref[...]), across)
    other = m ^ 1
    acc_ref[...] += dot(joined(three_ref[0]), weights(other))
    acc_ref[...] += dot(joined(three_ref[1]), weights(other - 2))
    acc_ref[...] += dot(joined(three_ref[2]), weights(other + 2))
    acc_ref[...] += dot(joined(far_ref[...]), weights(other + 4))
    out_ref[0:512, :] = packed_hidden(acc_ref[...])
    out_ref[512:576, :] = common_ref[...]


def down_body(m_ref, own_ref, left_ref, right_ref, far_ref, partner_ref, w_ref, out_ref, common_ref):
    m = m_ref[0]
    low = iota((576, LANES), 1) < 64
    low_w = iota((256, LANES), 1) < 64
    tops, bottoms, mats, commons = [], [], [], []
    mine = (own_ref, left_ref, right_ref, far_ref)
    for i, shift in enumerate((0, -2, 2, 4)):
        a = mine[i][...].astype(f32)
        b = partner_ref[i].astype(f32)
        tops.append(jnp.where(low, a, half_roll(b)).astype(bf16))
        bottoms.append(jnp.where(low, half_roll(a), b).astype(bf16))
        q = (m + shift) & 7
        wa = w_ref[q].astype(f32)
        wb = w_ref[q ^ 1].astype(f32)
        first = jnp.where(low_w, wa, half_roll(wb)).astype(bf16)
        second = jnp.where(low_w, half_roll(wa), wb).astype(bf16)
        for base, into in ((0, mats), (128, commons)):
            parts = []
            for f in range(8):
                at = slice(base + 16 * f, base + 16 * f + 16)
                parts += [first[at], second[at]]
            into.append(jnp.concatenate(parts, axis=0))
    top = jnp.concatenate(tops, axis=1)
    bottom = jnp.concatenate(bottoms, axis=1)
    mat = jnp.concatenate(mats, axis=1)
    common = jnp.concatenate(commons, axis=1)
    for i, rows in enumerate((top, bottom)):
        r = dot_nt(rows[:512], mat).astype(bf16)
        at = slice(32 * i, 32 * i + 32)
        out_ref[at, 0:16, :] = r[:, :LANES].reshape(32, 16, LANES)
        out_ref[at, 16:32, :] = r[:, LANES:].reshape(32, 16, LANES)
        common_ref[64 * i : 64 * i + 64, :] = dot_nt(rows[512:576], common)


def mixing_body(pos_ref, ids_ref, weight_ref, hi_ref, lo_ref):
    experts = iota((E, TOK), 0)
    w = jnp.zeros((E, TOK), f32)
    for k in range(TOP_K):
        w = jnp.where(ids_ref[k : k + 1, :] == experts, weight_ref[k : k + 1, :], w)
    pos = jnp.transpose(pos_ref[...]).astype(bf16)
    w = jnp.transpose(w)
    expand = jnp.where(iota((E, ROWS), 0) == (iota((E, ROWS), 1) >> 4), 1.0, 0.0).astype(bf16)
    hit = dot(pos, expand) == (iota((TOK, ROWS), 1) & 15).astype(f32)
    hi = w.astype(bf16)
    lo = (w - hi.astype(f32)).astype(bf16)
    hi_ref[...] = jnp.where(hit, dot(hi, expand), 0.0).astype(bf16)
    lo_ref[...] = jnp.where(hit, dot(lo, expand), 0.0).astype(bf16)


def combine_body(hi_ref, lo_ref, got_ref, common_ref, out_ref):
    hi, lo = hi_ref[...], lo_ref[...]
    for h in range(2):
        rows = got_ref[:, 16 * h : 16 * h + 16, :].reshape(ROWS, LANES)
        at = slice(LANES * h, LANES * h + LANES)
        out_ref[:, at] = (dot(hi, rows) + dot(lo, rows) + common_ref[:, at]).astype(bf16)


def serve_body(base):
    def body(w_ref, g_ref, u_ref, d_ref):
        low = iota((LANES, LANES), 1) < 64
        for i in range(16):
            block = w_ref[4 * i : 4 * i + 4, base : base + 32, :].reshape(LANES, LANES).astype(f32)
            turned = jnp.transpose(block).astype(bf16)
            at = slice(LANES * i, LANES * i + LANES)
            g_ref[:, at] = turned[:64]
            u_ref[:, at] = turned[64:]
        for i in range(8):
            sides = []
            for s in range(2):
                straight, rolled = [], []
                for f in range(4):
                    x = w_ref[8 * i + 4 * s + f, base + 32 : base + 48, :].astype(f32)
                    y = half_roll(x)
                    straight += [x, y]
                    rolled += [y, x]
                sides.append(jnp.concatenate(rolled if s else straight, axis=0))
            turned = jnp.transpose(jnp.where(low, sides[0], sides[1])).astype(bf16)
            at = 256 * i
            d_ref[:, at : at + LANES] = turned[:64]
            d_ref[:, at + LANES : at + 2 * LANES] = turned[64:]

    return body


def shift(x, step):
    return lax.ppermute(x, "tp", [(i, (i + step) % N_TP) for i in range(N_TP)])


def swap(x, k):
    return lax.ppermute(x, "tp", [(i, i ^ k) for i in range(N_TP)])


def shape(*dims, dtype=bf16):
    return jax.ShapeDtypeStruct(dims, dtype)


def local(
    prompt,
    norm_gain,
    gate_train,
    up_train,
    down_train,
    common_gate_train,
    common_up_train,
    common_down_train,
    route_ids,
    route_weights,
):
    m = lax.axis_index("tp").astype(jnp.int32).reshape(1)
    ids = route_ids.T
    route_weights = route_weights.T
    gain = norm_gain.reshape(1, W32)

    send, normed, pos = call(
        dispatch_body, (shape(64, 80, LANES), shape(TOK, D), shape(E, TOK, dtype=f32)), 7, 1, far=range(8), keep=(1, 2)
    )(m, prompt, ids, gain, common_gate_train, common_up_train, common_down_train)
    got = lax.all_to_all(send, "fs", 0, 0, tiled=True)

    pieces = call(prepare_body, tuple(shape(8, 48, LANES) for _ in range(N_TP)), 5, 1, far=range(8))(
        m, gain, gate_train, up_train, down_train
    )
    crossed = [pieces[0]] + [swap(pieces[k], k) for k in range(1, N_TP)]
    spread = call(assemble_body, shape(64, 48, LANES), 9, 1, keep=())(m, *crossed)
    weights = lax.all_to_all(spread, "fs", 0, 0, tiled=True)

    own = got[:, 0:32, :]
    left = shift(own, 2)
    right = shift(own, -2)
    far_a = shift(left[:32], 2)
    far_b = shift(right[32:], -2)
    three = swap(jnp.stack([own, left, right]), 1)
    far = swap(jnp.concatenate([far_a, far_b]), 1)

    common_hidden = call(common_hidden_body, shape(64, LANES), 2)(normed, got)
    mix_hi, mix_lo = call(mixing_body, (shape(TOK, ROWS), shape(TOK, ROWS)), 3, far=(1, 2))(pos, ids, route_weights)

    down_send = jnp.concatenate(
        [weights[:, 32:48, :].reshape(8, 128, LANES), got[:, 64:80, :].reshape(8, 128, LANES)], axis=1
    )
    down_got = lax.all_to_all(down_send, "tp", 0, 0, tiled=True)

    hidden = call(
        hidden_body, shape(576, LANES), 10, 1, [pltpu.VMEM((ROWS, LANES), f32)]
    )(m, own, left, right, far_a, far_b, three, far, weights, common_hidden)
    h_left = shift(hidden, 2)
    h_right = shift(hidden, -2)
    h_far = shift(hidden, 4)
    partner = swap(jnp.stack([hidden, h_left, h_right, h_far]), 1)

    expert_out, common_out = call(
        down_body, (shape(64, 32, LANES), shape(TOK, COLS, dtype=f32)), 7, 1, keep=(1,)
    )(m, hidden, h_left, h_right, h_far, partner, down_got)
    returned = lax.all_to_all(expert_out, "fs", 0, 0, tiled=True)

    serve = tuple(shape(U, D) for _ in range(3))
    gate_serve, up_serve, down_serve = call(serve_body(0), serve, 1, keep=())(weights)
    commons = call(serve_body(32), serve, 1, keep=())(got)

    mixture = call(combine_body, shape(TOK, COLS), 4, keep=())(mix_hi, mix_lo, returned, common_out)
    return (mixture, gate_serve[None], up_serve[None], down_serve[None], *commons)


def solution(mesh):
    in_specs = (
        P("fs", None),
        P("fs"),
        P("fs", "tp"),
        P("fs", "tp"),
        P("fs", "tp"),
        P("fs", "tp"),
        P("fs", "tp"),
        P("fs", "tp"),
        P("fs", None),
        P("fs", None),
    )
    out_specs = (
        P("fs", "tp"),
        P("fs", "tp", None),
        P("fs", "tp", None),
        P("fs", "tp", None),
        P("tp", None),
        P("tp", None),
        P("tp", None),
    )

    return jax.shard_map(local, mesh=mesh, in_specs=in_specs, out_specs=out_specs, check_vma=False)
```

```python
import jax
import jax.numpy as jnp
from jax import lax
from jax.experimental import pallas as pl
from jax.experimental.pallas import tpu as pltpu
from jax.sharding import PartitionSpec as P


E = 64
CAP = 16
TOP_K = 6
TOK = 128
D = 2048
N_FS = 64
N_TP = 8
U = 64
W32 = D // N_FS
COLS = D // N_TP
ROWS = E * CAP
LANES = 128
epsilon = 1e-06

f32 = jnp.float32
bf16 = jnp.bfloat16
VM = pl.BlockSpec(memory_space=pltpu.VMEM)
SM = pl.BlockSpec(memory_space=pltpu.SMEM)


def iota(shape, dim):
    return lax.broadcasted_iota(jnp.int32, shape, dim)


def half_roll(x):
    return pltpu.roll(x, 64, 1)


def call(body, outs, n_in, smem=0, scratch=(), far=(), keep=True):
    flat, tree = jax.tree.flatten(outs)
    kept = [pltpu.VMEM(o.shape, o.dtype) if keep is True or i in keep else pltpu.HBM(o.shape, o.dtype) for i, o in enumerate(flat)]
    fn = pl.pallas_call(
        body,
        out_shape=jax.tree.unflatten(tree, kept),
        in_specs=[SM] * smem + [VM] * (n_in - smem),
        out_specs=jax.tree.map(lambda _: VM, outs),
        scratch_shapes=list(scratch),
        compiler_params=pltpu.CompilerParams(vmem_limit_bytes=16 * 2**20),
    )

    def run(*args):
        placed = [
            a if i < smem else pltpu.with_memory_space_constraint(a, pltpu.HBM if i in far else pltpu.VMEM)
            for i, a in enumerate(args)
        ]
        return fn(*placed)

    return run


def dot(a, b):
    return jnp.dot(a, b, preferred_element_type=f32)


def dot_nt(a, b):
    return lax.dot_general(a, b, (((1,), (1,)), ((), ())), preferred_element_type=f32)


def gain_column(gain_ref):
    n = gain_ref.shape[1]
    eye = iota((n, n), 0) == iota((n, n), 1)
    spread = jnp.where(eye, jnp.broadcast_to(gain_ref[...], (n, n)), 0.0)
    return jnp.sum(spread, axis=1, keepdims=True)


def dispatch_body(m_ref, prompt_ref, ids_ref, gain_ref, cg_ref, cu_ref, cd_ref, send_ref, normed_ref, pos_ref):
    m = m_ref[0]
    values = prompt_ref[...].astype(f32)
    scale = lax.rsqrt(jnp.mean(values * values, axis=1, keepdims=True) + epsilon)
    normed_ref[...] = (values * scale).astype(bf16)
    experts = iota((E, TOK), 0)
    named = jnp.zeros((E, TOK), f32)
    for k in range(TOP_K):
        named = jnp.where(ids_ref[k : k + 1, :] == experts, 1.0, named)
    earlier = jnp.where(iota((TOK, TOK), 0) < iota((TOK, TOK), 1), 1.0, 0.0).astype(bf16)
    slot = dot(named.astype(bf16), earlier)
    pos = jnp.where(named > 0.0, slot, -1.0)
    pos_ref[...] = pos
    expand = jnp.where((iota((ROWS, E), 0) >> 4) == iota((ROWS, E), 1), 1.0, 0.0).astype(bf16)
    at = dot(expand, pos.astype(bf16))
    pick = jnp.where(at == (iota((ROWS, TOK), 0) & 15).astype(f32), 1.0, 0.0).astype(bf16)
    mine = normed_ref[:, pl.ds(pl.multiple_of(m * COLS, COLS), COLS)]
    rows = dot(pick, mine).astype(bf16)
    send_ref[:, 0:16, :] = rows[:, :LANES].reshape(E, CAP, LANES)
    send_ref[:, 16:32, :] = rows[:, LANES:].reshape(E, CAP, LANES)
    gain = gain_column(gain_ref)
    both = jnp.concatenate([cg_ref[...] * gain, cu_ref[...] * gain], axis=1)
    down = jnp.concatenate([cd_ref[0:16, :], cd_ref[16:32, :]], axis=1)
    piece = jnp.concatenate([both, down], axis=0).astype(bf16)
    send_ref[:, 32:80, :] = jnp.broadcast_to(piece[None], (N_FS, 48, LANES))


def prepare_body(m_ref, gain_ref, g_ref, u_ref, d_ref, *out_refs):
    m = m_ref[0]
    gain = gain_column(gain_ref)
    low = iota((W32, LANES), 1) < 64
    low16 = iota((16, LANES), 1) < 64
    for k in range(N_TP):
        to = m ^ k
        odd = (to & 1) == 1
        for j in range(8):
            at = pl.ds(pl.multiple_of(j * 512 + (to >> 1) * LANES, LANES), LANES)
            g = g_ref[:, at] * gain
            u = u_ref[:, at] * gain
            d = d_ref[:, at]
            g = jnp.where(odd, half_roll(g), g)
            u = jnp.where(odd, u, half_roll(u))
            out_refs[k][j, 0:32, :] = jnp.where(low, g, u).astype(bf16)
            d0, d1 = d[0:16, :], d[16:32, :]
            d0 = jnp.where(odd, half_roll(d0), d0)
            d1 = jnp.where(odd, d1, half_roll(d1))
            out_refs[k][j, 32:48, :] = jnp.where(low16, d0, d1).astype(bf16)


def assemble_body(m_ref, *refs):
    m = m_ref[0]
    out_ref = refs[-1]
    for k in range(N_TP):
        out_ref[pl.ds(pl.multiple_of((m ^ k) * 8, 8), 8)] = refs[k][...]


def silu(v):
    return v / (1.0 + jnp.exp(-v))


def packed_hidden(acc):
    half = acc.shape[0] // 2
    top, bottom = acc[:half], acc[half:]
    first = silu(top) * half_roll(top)
    second = silu(half_roll(bottom)) * bottom
    return jnp.where(iota((half, LANES), 1) < 64, first, second).astype(bf16)


def common_hidden_body(normed_ref, got_ref, out_ref):
    weights = got_ref[:, 32:64, :].reshape(D, LANES)
    out_ref[...] = packed_hidden(dot(normed_ref[...], weights))


def copy_body(*refs):
    out_ref, at = refs[-1], 0
    for ref in refs[:-1]:
        out_ref[at : at + ref.shape[0]] = ref[...]
        at += ref.shape[0]


def part_body(at):
    def body(in_ref, out_ref):
        out_ref[...] = in_ref[at : at + out_ref.shape[0]]

    return body


def own_rows_body(got_ref, out_ref):
    out_ref[...] = got_ref[:, 0:32, :]


def down_block(w_ref, got_ref, q):
    at = pl.ds(pl.multiple_of((q & 7) * 8, 8), 8)
    return w_ref[at, 32:48, :].reshape(LANES, LANES), got_ref[at, 64:80, :].reshape(LANES, LANES)


H_ROWS = 576
PIECE = 256
MESSAGE = H_ROWS + 2 * PIECE


def hidden_body(m_ref, own_ref, left_ref, right_ref, across_ref, three_ref, far_ref, w_ref, got_ref, common_ref, *rest):
    m = m_ref[0]
    to_refs, acc_ref = rest[:4], rest[4]

    def joined(x):
        n = x.shape[0]
        return jnp.concatenate([x[:, 0:16, :].reshape(n * 16, LANES), x[:, 16:32, :].reshape(n * 16, LANES)], axis=1)

    def weights(q):
        return w_ref[pl.ds(pl.multiple_of((q & 7) * 8, 8), 8), 0:32, :].reshape(COLS, LANES)

    acc_ref[...] = dot(joined(own_ref[...]), weights(m))
    acc_ref[...] += dot(joined(left_ref[...]), weights(m - 2))
    acc_ref[...] += dot(joined(right_ref[...]), weights(m + 2))
    acc_ref[...] += dot(joined(across_ref[...]), weights(m + 4))
    other = m ^ 1
    acc_ref[...] += dot(joined(three_ref[0:64]), weights(other))
    acc_ref[...] += dot(joined(three_ref[64:128]), weights(other - 2))
    acc_ref[...] += dot(joined(three_ref[128:192]), weights(other + 2))
    acc_ref[...] += dot(joined(far_ref[...]), weights(other + 4))
    hidden = packed_hidden(acc_ref[...])
    for ref in to_refs:
        ref[0:512, :] = hidden
        ref[512:H_ROWS, :] = common_ref[...]
    for ref, step in zip(to_refs, (0, 2, -2, 4)):
        for i, q in enumerate((m + step, (m + step) ^ 1)):
            at = H_ROWS + PIECE * i
            routed, shared = down_block(w_ref, got_ref, q)
            ref[at : at + LANES, :] = routed
            ref[at + LANES : at + PIECE, :] = shared


def pair_body(own_ref, left_ref, right_ref, far_ref, out_ref):
    for i, ref in enumerate((own_ref, left_ref, right_ref, far_ref)):
        out_ref[i, 0:H_ROWS, :] = ref[0:H_ROWS, :]
        out_ref[i, H_ROWS : H_ROWS + PIECE, :] = ref[H_ROWS + PIECE : MESSAGE, :]


def down_body(own_ref, left_ref, right_ref, far_ref, partner_ref, out_ref, common_ref):
    low = iota((H_ROWS, LANES), 1) < 64
    low_w = iota((PIECE, LANES), 1) < 64
    tops, bottoms, mats, commons = [], [], [], []
    for i, ref in enumerate((own_ref, left_ref, right_ref, far_ref)):
        a = ref[0:H_ROWS, :].astype(f32)
        b = partner_ref[i, 0:H_ROWS, :].astype(f32)
        tops.append(jnp.where(low, a, half_roll(b)).astype(bf16))
        bottoms.append(jnp.where(low, half_roll(a), b).astype(bf16))
        wa = ref[H_ROWS : H_ROWS + PIECE, :].astype(f32)
        wb = partner_ref[i, H_ROWS : H_ROWS + PIECE, :].astype(f32)
        first = jnp.where(low_w, wa, half_roll(wb)).astype(bf16)
        second = jnp.where(low_w, half_roll(wa), wb).astype(bf16)
        for base, into in ((0, mats), (128, commons)):
            parts = []
            for f in range(8):
                at = slice(base + 16 * f, base + 16 * f + 16)
                parts += [first[at], second[at]]
            into.append(jnp.concatenate(parts, axis=0))
    top = jnp.concatenate(tops, axis=1)
    bottom = jnp.concatenate(bottoms, axis=1)
    mat = jnp.concatenate(mats, axis=1)
    common = jnp.concatenate(commons, axis=1)
    for i, rows in enumerate((top, bottom)):
        r = dot_nt(rows[:512], mat).astype(bf16)
        at = slice(32 * i, 32 * i + 32)
        out_ref[at, 0:16, :] = r[:, :LANES].reshape(32, 16, LANES)
        out_ref[at, 16:32, :] = r[:, LANES:].reshape(32, 16, LANES)
        common_ref[64 * i : 64 * i + 64, :] = dot_nt(rows[512:576], common)


def mixing_body(pos_ref, ids_ref, weight_ref, hi_ref, lo_ref):
    experts = iota((E, TOK), 0)
    w = jnp.zeros((E, TOK), f32)
    for k in range(TOP_K):
        w = jnp.where(ids_ref[k : k + 1, :] == experts, weight_ref[k : k + 1, :], w)
    pos = jnp.transpose(pos_ref[...]).astype(bf16)
    w = jnp.transpose(w)
    expand = jnp.where(iota((E, ROWS), 0) == (iota((E, ROWS), 1) >> 4), 1.0, 0.0).astype(bf16)
    hit = dot(pos, expand) == (iota((TOK, ROWS), 1) & 15).astype(f32)
    hi = w.astype(bf16)
    lo = (w - hi.astype(f32)).astype(bf16)
    hi_ref[...] = jnp.where(hit, dot(hi, expand), 0.0).astype(bf16)
    lo_ref[...] = jnp.where(hit, dot(lo, expand), 0.0).astype(bf16)


def combine_body(hi_ref, lo_ref, got_ref, common_ref, out_ref):
    hi, lo = hi_ref[...], lo_ref[...]
    for h in range(2):
        rows = got_ref[:, 16 * h : 16 * h + 16, :].reshape(ROWS, LANES)
        at = slice(LANES * h, LANES * h + LANES)
        out_ref[:, at] = (dot(hi, rows) + dot(lo, rows) + common_ref[:, at]).astype(bf16)


def serve_body(base):
    def body(w_ref, g_ref, u_ref, d_ref):
        low = iota((LANES, LANES), 1) < 64
        for i in range(16):
            block = w_ref[4 * i : 4 * i + 4, base : base + 32, :].reshape(LANES, LANES).astype(f32)
            turned = jnp.transpose(block).astype(bf16)
            at = slice(LANES * i, LANES * i + LANES)
            g_ref[:, at] = turned[:64]
            u_ref[:, at] = turned[64:]
        for i in range(8):
            sides = []
            for s in range(2):
                straight, rolled = [], []
                for f in range(4):
                    x = w_ref[8 * i + 4 * s + f, base + 32 : base + 48, :].astype(f32)
                    y = half_roll(x)
                    straight += [x, y]
                    rolled += [y, x]
                sides.append(jnp.concatenate(rolled if s else straight, axis=0))
            turned = jnp.transpose(jnp.where(low, sides[0], sides[1])).astype(bf16)
            at = 256 * i
            d_ref[:, at : at + LANES] = turned[:64]
            d_ref[:, at + LANES : at + 2 * LANES] = turned[64:]

    return body


def shift(x, step):
    return lax.ppermute(x, "tp", [(i, (i + step) % N_TP) for i in range(N_TP)])


def swap(x, k):
    return lax.ppermute(x, "tp", [(i, i ^ k) for i in range(N_TP)])


def shape(*dims, dtype=bf16):
    return jax.ShapeDtypeStruct(dims, dtype)


def local(
    prompt,
    norm_gain,
    gate_train,
    up_train,
    down_train,
    common_gate_train,
    common_up_train,
    common_down_train,
    route_ids,
    route_weights,
):
    m = lax.axis_index("tp").astype(jnp.int32).reshape(1)
    ids = route_ids.T
    route_weights = route_weights.T
    gain = norm_gain.reshape(1, W32)

    send, normed, pos = call(
        dispatch_body, (shape(64, 80, LANES), shape(TOK, D), shape(E, TOK, dtype=f32)), 7, 1, far=range(8), keep=(2,)
    )(m, prompt, ids, gain, common_gate_train, common_up_train, common_down_train)
    got = lax.all_to_all(send, "fs", 0, 0, tiled=True)

    pieces = call(prepare_body, tuple(shape(8, 48, LANES) for _ in range(N_TP)), 5, 1, far=range(8))(
        m, gain, gate_train, up_train, down_train
    )
    crossed = [pieces[0]] + [swap(pieces[k], k) for k in range(1, N_TP)]
    spread = call(assemble_body, shape(64, 48, LANES), 9, 1, keep=())(m, *crossed)
    weights = lax.all_to_all(spread, "fs", 0, 0, tiled=True)

    own = call(own_rows_body, shape(64, 32, LANES), 1)(got)
    left = shift(own, 2)
    right = shift(own, -2)
    far_a = shift(call(part_body(0), shape(32, 32, LANES), 1)(left), 2)
    far_b = shift(call(part_body(32), shape(32, 32, LANES), 1)(right), -2)
    three = call(copy_body, shape(192, 32, LANES), 3)(own, left, right)
    three = swap(three, 1)
    across = call(copy_body, shape(64, 32, LANES), 2)(far_a, far_b)
    far = swap(across, 1)

    common_hidden = call(common_hidden_body, shape(64, LANES), 2, far=(0,))(normed, got)
    mix_hi, mix_lo = call(mixing_body, (shape(TOK, ROWS), shape(TOK, ROWS)), 3, far=(1, 2), keep=())(
        pos, ids, route_weights
    )

    mine, to_right, to_left, to_far = call(
        hidden_body,
        tuple(shape(MESSAGE, LANES) for _ in range(4)),
        10,
        1,
        [pltpu.VMEM((ROWS, LANES), f32)],
        far=(3, 4, 5, 6),
    )(m, own, left, right, across, three, far, weights, got, common_hidden)
    h_left = shift(to_right, 2)
    h_right = shift(to_left, -2)
    h_far = shift(to_far, 4)
    pair = call(pair_body, shape(4, H_ROWS + PIECE, LANES), 4)(mine, h_left, h_right, h_far)
    partner = swap(pair, 1)

    expert_out, common_out = call(
        down_body, (shape(64, 32, LANES), shape(TOK, COLS, dtype=f32)), 5
    )(mine, h_left, h_right, h_far, partner)
    returned = lax.all_to_all(expert_out, "fs", 0, 0, tiled=True)

    serve = tuple(shape(U, D) for _ in range(3))
    gate_serve, up_serve, down_serve = call(serve_body(0), serve, 1, keep=())(weights)
    commons = call(serve_body(32), serve, 1, keep=())(got)

    mixture = call(combine_body, shape(TOK, COLS), 4, far=(0, 1), keep=())(mix_hi, mix_lo, returned, common_out)
    return (mixture, gate_serve[None], up_serve[None], down_serve[None], *commons)


def solution(mesh):
    in_specs = (
        P("fs", None),
        P("fs"),
        P("fs", "tp"),
        P("fs", "tp"),
        P("fs", "tp"),
        P("fs", "tp"),
        P("fs", "tp"),
        P("fs", "tp"),
        P("fs", None),
        P("fs", None),
    )
    out_specs = (
        P("fs", "tp"),
        P("fs", "tp", None),
        P("fs", "tp", None),
        P("fs", "tp", None),
        P("tp", None),
        P("tp", None),
        P("tp", None),
    )

    return jax.shard_map(local, mesh=mesh, in_specs=in_specs, out_specs=out_specs, check_vma=False)
```

```python
import jax
import jax.numpy as jnp
from jax import lax
from jax.experimental import pallas as pl
from jax.experimental.pallas import tpu as pltpu
from jax.sharding import PartitionSpec as P


E = 64
CAP = 16
TOP_K = 6
TOK = 128
D = 2048
N_FS = 64
N_TP = 8
U = 64
W32 = D // N_FS
COLS = D // N_TP
ROWS = E * CAP
LANES = 128
PARTS = 8
COLUMNS = [[8 * z + y for y in range(8)] for z in range(8)]
epsilon = 1e-06

f32 = jnp.float32
bf16 = jnp.bfloat16
VM = pl.BlockSpec(memory_space=pltpu.VMEM)
SM = pl.BlockSpec(memory_space=pltpu.SMEM)


def iota(shape, dim):
    return lax.broadcasted_iota(jnp.int32, shape, dim)


def half_roll(x):
    return pltpu.roll(x, 64, 1)


def call(body, outs, n_in, smem=0, scratch=(), far=(), keep=True):
    flat, tree = jax.tree.flatten(outs)
    kept = [pltpu.VMEM(o.shape, o.dtype) if keep is True or i in keep else pltpu.HBM(o.shape, o.dtype) for i, o in enumerate(flat)]
    fn = pl.pallas_call(
        body,
        out_shape=jax.tree.unflatten(tree, kept),
        in_specs=[SM] * smem + [VM] * (n_in - smem),
        out_specs=jax.tree.map(lambda _: VM, outs),
        scratch_shapes=list(scratch),
        compiler_params=pltpu.CompilerParams(vmem_limit_bytes=16 * 2**20),
    )

    def run(*args):
        placed = [
            a if i < smem else pltpu.with_memory_space_constraint(a, pltpu.HBM if i in far else pltpu.VMEM)
            for i, a in enumerate(args)
        ]
        return fn(*placed)

    return run


def dot(a, b):
    return jnp.dot(a, b, preferred_element_type=f32)


def dot_nt(a, b):
    return lax.dot_general(a, b, (((1,), (1,)), ((), ())), preferred_element_type=f32)


def gain_column(gain_ref):
    n = gain_ref.shape[1]
    eye = iota((n, n), 0) == iota((n, n), 1)
    spread = jnp.where(eye, jnp.broadcast_to(gain_ref[...], (n, n)), 0.0)
    return jnp.sum(spread, axis=1, keepdims=True)


def dispatch_body(m_ref, prompt_ref, ids_ref, gain_ref, cg_ref, cu_ref, cd_ref, send_ref, normed_ref, pos_ref):
    m = m_ref[0]
    gain = gain_column(gain_ref)
    both = jnp.concatenate([cg_ref[...] * gain, cu_ref[...] * gain], axis=1)
    down = jnp.concatenate([cd_ref[0:16, :], cd_ref[16:32, :]], axis=1)
    piece = jnp.concatenate([both, down, jnp.zeros((16, LANES), f32)], axis=0)
    parts = piece.reshape(PARTS, 8, LANES).astype(bf16)
    for z in range(N_FS // PARTS):
        send_ref[PARTS * z : PARTS * z + PARTS, 32:40, :] = parts
    values = prompt_ref[...].astype(f32)
    scale = lax.rsqrt(jnp.mean(values * values, axis=1, keepdims=True) + epsilon)
    normed_ref[...] = (values * scale).astype(bf16)
    experts = iota((E, TOK), 0)
    named = jnp.zeros((E, TOK), f32)
    for k in range(TOP_K):
        named = jnp.where(ids_ref[k : k + 1, :] == experts, 1.0, named)
    earlier = jnp.where(iota((TOK, TOK), 0) < iota((TOK, TOK), 1), 1.0, 0.0).astype(bf16)
    slot = dot(named.astype(bf16), earlier)
    pos = jnp.where(named > 0.0, slot, -1.0)
    pos_ref[...] = pos
    expand = jnp.where((iota((ROWS, E), 0) >> 4) == iota((ROWS, E), 1), 1.0, 0.0).astype(bf16)
    at = dot(expand, pos.astype(bf16))
    pick = jnp.where(at == (iota((ROWS, TOK), 0) & 15).astype(f32), 1.0, 0.0).astype(bf16)
    mine = normed_ref[:, pl.ds(pl.multiple_of(m * COLS, COLS), COLS)]
    rows = dot(pick, mine).astype(bf16)
    send_ref[:, 0:16, :] = rows[:, :LANES].reshape(E, CAP, LANES)
    send_ref[:, 16:32, :] = rows[:, LANES:].reshape(E, CAP, LANES)


def split_body(got_ref, own_ref, parts_ref):
    own_ref[...] = got_ref[:, 0:32, :]
    parts = got_ref[:, 32:40, :]
    for y in range(PARTS):
        parts_ref[y] = parts


def join_body(parts_ref, out_ref):
    pieces = [parts_ref[p].astype(f32) for p in range(6)]
    out_ref[...] = jnp.concatenate(pieces, axis=1).astype(bf16)


STEPS = (0, 2, -2, 4)


def prepare_body(m_ref, gain_ref, g_ref, u_ref, d_ref, keep_ref, swap_ref):
    m = m_ref[0]
    gain = gain_column(gain_ref)
    low = iota((W32, LANES), 1) < 64
    low16 = iota((16, LANES), 1) < 64
    for i, step in enumerate(STEPS):
        for out_ref, to in ((keep_ref, (m + step) & 7), (swap_ref, ((m + step) & 7) ^ 1)):
            odd = (to & 1) == 1
            for j in range(8):
                at = pl.ds(pl.multiple_of(j * 512 + (to >> 1) * LANES, LANES), LANES)
                g = g_ref[:, at] * gain
                u = u_ref[:, at] * gain
                d = d_ref[:, at]
                g = jnp.where(odd, half_roll(g), g)
                u = jnp.where(odd, u, half_roll(u))
                out_ref[i, j, 0:32, :] = jnp.where(low, g, u).astype(bf16)
                d0, d1 = d[0:16, :], d[16:32, :]
                d0 = jnp.where(odd, half_roll(d0), d0)
                d1 = jnp.where(odd, d1, half_roll(d1))
                out_ref[i, j, 32:48, :] = jnp.where(low16, d0, d1).astype(bf16)


def repack_body(keep_ref, swapped_ref, *out_refs):
    for i, out_ref in enumerate(out_refs):
        out_ref[0:8] = keep_ref[i + 1]
        out_ref[8:16] = swapped_ref[i + 1]


def assemble_body(m_ref, keep_ref, swapped_ref, left_ref, right_ref, far_ref, out_ref):
    m = m_ref[0]

    def put(t, x):
        out_ref[pl.ds(pl.multiple_of(t * 8, 8), 8)] = x

    put(m, keep_ref[0])
    put(m ^ 1, swapped_ref[0])
    for step, ref in zip(STEPS[1:], (left_ref, right_ref, far_ref)):
        t = (m - step) & 7
        put(t, ref[0:8])
        put(t ^ 1, ref[8:16])


def silu(v):
    return v / (1.0 + jnp.exp(-v))


def packed_hidden(acc):
    half = acc.shape[0] // 2
    top, bottom = acc[:half], acc[half:]
    first = silu(top) * half_roll(top)
    second = silu(half_roll(bottom)) * bottom
    return jnp.where(iota((half, LANES), 1) < 64, first, second).astype(bf16)


def copy_body(*refs):
    out_ref, at = refs[-1], 0
    for ref in refs[:-1]:
        out_ref[at : at + ref.shape[0]] = ref[...]
        at += ref.shape[0]


def part_body(at):
    def body(in_ref, out_ref):
        out_ref[...] = in_ref[at : at + out_ref.shape[0]]

    return body


def down_block(w_ref, q):
    return w_ref[pl.ds(pl.multiple_of((q & 7) * 8, 8), 8), 32:48, :].reshape(LANES, LANES)


def write_messages(m, rows, w_ref, refs):
    n = rows.shape[0]
    for ref, step in zip(refs, STEPS):
        ref[0:n, :] = rows
        ref[n : n + LANES, :] = down_block(w_ref, m + step)
        ref[n + LANES : n + 2 * LANES, :] = down_block(w_ref, (m + step) ^ 1)


def common_hidden_body(m_ref, normed_ref, w_ref, *to_refs):
    weights = w_ref[:, 0:32, :].reshape(D, LANES)
    write_messages(m_ref[0], packed_hidden(dot(normed_ref[...], weights)), w_ref, to_refs)


def hidden_body(m_ref, own_ref, left_ref, right_ref, across_ref, three_ref, far_ref, w_ref, *rest):
    m = m_ref[0]
    to_refs, acc_ref = rest[:4], rest[4]

    def joined(x):
        n = x.shape[0]
        return jnp.concatenate([x[:, 0:16, :].reshape(n * 16, LANES), x[:, 16:32, :].reshape(n * 16, LANES)], axis=1)

    def weights(q):
        return w_ref[pl.ds(pl.multiple_of((q & 7) * 8, 8), 8), 0:32, :].reshape(COLS, LANES)

    acc_ref[...] = dot(joined(own_ref[...]), weights(m))
    acc_ref[...] += dot(joined(left_ref[...]), weights(m - 2))
    acc_ref[...] += dot(joined(right_ref[...]), weights(m + 2))
    acc_ref[...] += dot(joined(across_ref[...]), weights(m + 4))
    other = m ^ 1
    acc_ref[...] += dot(joined(three_ref[0:64]), weights(other))
    acc_ref[...] += dot(joined(three_ref[64:128]), weights(other - 2))
    acc_ref[...] += dot(joined(three_ref[128:192]), weights(other + 2))
    acc_ref[...] += dot(joined(far_ref[...]), weights(other + 4))
    write_messages(m, packed_hidden(acc_ref[...]), w_ref, to_refs)


def pair_body(*refs):
    out_ref = refs[-1]
    n = out_ref.shape[1] - LANES
    for i, ref in enumerate(refs[:-1]):
        out_ref[i, 0:n, :] = ref[0:n, :]
        out_ref[i, n : n + LANES, :] = ref[n + LANES : n + 2 * LANES, :]


def down_parts(refs, partner_ref):
    n = partner_ref.shape[1] - LANES
    low = iota((n, LANES), 1) < 64
    low_w = iota((LANES, LANES), 1) < 64
    tops, bottoms, mats = [], [], []
    for i, ref in enumerate(refs):
        a = ref[0:n, :].astype(f32)
        b = partner_ref[i, 0:n, :].astype(f32)
        tops.append(jnp.where(low, a, half_roll(b)).astype(bf16))
        bottoms.append(jnp.where(low, half_roll(a), b).astype(bf16))
        wa = ref[n : n + LANES, :].astype(f32)
        wb = partner_ref[i, n : n + LANES, :].astype(f32)
        first = jnp.where(low_w, wa, half_roll(wb)).astype(bf16)
        second = jnp.where(low_w, half_roll(wa), wb).astype(bf16)
        parts = []
        for f in range(8):
            at = slice(16 * f, 16 * f + 16)
            parts += [first[at], second[at]]
        mats.append(jnp.concatenate(parts, axis=0))
    return tuple(jnp.concatenate(x, axis=1) for x in (tops, bottoms, mats))


def down_body(own_ref, left_ref, right_ref, far_ref, partner_ref, out_ref):
    top, bottom, mat = down_parts((own_ref, left_ref, right_ref, far_ref), partner_ref)
    for i, rows in enumerate((top, bottom)):
        r = dot_nt(rows, mat).astype(bf16)
        at = slice(32 * i, 32 * i + 32)
        out_ref[at, 0:16, :] = r[:, :LANES].reshape(32, 16, LANES)
        out_ref[at, 16:32, :] = r[:, LANES:].reshape(32, 16, LANES)


def common_down_body(own_ref, left_ref, right_ref, far_ref, partner_ref, out_ref):
    top, bottom, mat = down_parts((own_ref, left_ref, right_ref, far_ref), partner_ref)
    out_ref[0:64, :] = dot_nt(top, mat)
    out_ref[64:128, :] = dot_nt(bottom, mat)


def mixing_body(pos_ref, ids_ref, weight_ref, hi_ref, lo_ref):
    experts = iota((E, TOK), 0)
    w = jnp.zeros((E, TOK), f32)
    for k in range(TOP_K):
        w = jnp.where(ids_ref[k : k + 1, :] == experts, weight_ref[k : k + 1, :], w)
    pos = jnp.transpose(pos_ref[...]).astype(bf16)
    w = jnp.transpose(w)
    expand = jnp.where(iota((E, ROWS), 0) == (iota((E, ROWS), 1) >> 4), 1.0, 0.0).astype(bf16)
    hit = dot(pos, expand) == (iota((TOK, ROWS), 1) & 15).astype(f32)
    hi = w.astype(bf16)
    lo = (w - hi.astype(f32)).astype(bf16)
    hi_ref[...] = jnp.where(hit, dot(hi, expand), 0.0).astype(bf16)
    lo_ref[...] = jnp.where(hit, dot(lo, expand), 0.0).astype(bf16)


def combine_body(hi_ref, lo_ref, got_ref, common_ref, out_ref):
    hi, lo = hi_ref[...], lo_ref[...]
    for h in range(2):
        rows = got_ref[:, 16 * h : 16 * h + 16, :].reshape(ROWS, LANES)
        at = slice(LANES * h, LANES * h + LANES)
        out_ref[:, at] = (dot(hi, rows) + dot(lo, rows) + common_ref[:, at]).astype(bf16)


def serve_body(w_ref, g_ref, u_ref, d_ref):
    low = iota((LANES, LANES), 1) < 64
    for i in range(16):
        block = w_ref[4 * i : 4 * i + 4, 0:32, :].reshape(LANES, LANES).astype(f32)
        turned = jnp.transpose(block).astype(bf16)
        at = slice(LANES * i, LANES * i + LANES)
        g_ref[:, at] = turned[:64]
        u_ref[:, at] = turned[64:]
    for i in range(8):
        sides = []
        for s in range(2):
            straight, rolled = [], []
            for f in range(4):
                x = w_ref[8 * i + 4 * s + f, 32:48, :].astype(f32)
                y = half_roll(x)
                straight += [x, y]
                rolled += [y, x]
            sides.append(jnp.concatenate(rolled if s else straight, axis=0))
        turned = jnp.transpose(jnp.where(low, sides[0], sides[1])).astype(bf16)
        at = 256 * i
        d_ref[:, at : at + LANES] = turned[:64]
        d_ref[:, at + LANES : at + 2 * LANES] = turned[64:]


def shift(x, step):
    return lax.ppermute(x, "tp", [(i, (i + step) % N_TP) for i in range(N_TP)])


def swap(x, k):
    return lax.ppermute(x, "tp", [(i, i ^ k) for i in range(N_TP)])


def shape(*dims, dtype=bf16):
    return jax.ShapeDtypeStruct(dims, dtype)


def local(
    prompt,
    norm_gain,
    gate_train,
    up_train,
    down_train,
    common_gate_train,
    common_up_train,
    common_down_train,
    route_ids,
    route_weights,
):
    m = lax.axis_index("tp").astype(jnp.int32).reshape(1)
    ids = route_ids.T
    route_weights = route_weights.T
    gain = norm_gain.reshape(1, W32)

    send, normed, pos = call(
        dispatch_body, (shape(64, 40, LANES), shape(TOK, D), shape(E, TOK, dtype=f32)), 7, 1, far=range(8), keep=(2,)
    )(m, prompt, ids, gain, common_gate_train, common_up_train, common_down_train)
    got = lax.all_to_all(send, "fs", 0, 0, tiled=True)

    half = shape(4, 8, 48, LANES)
    kept, to_partner = call(prepare_body, (half, half), 5, 1, far=range(8))(m, gain, gate_train, up_train, down_train)
    swapped = swap(to_partner, 1)
    message = shape(16, 48, LANES)
    to_right, to_left, to_far = call(repack_body, (message, message, message), 2)(kept, swapped)
    w_far = shift(to_far, 4)
    w_left = shift(to_right, 2)
    w_right = shift(to_left, -2)
    spread = call(assemble_body, shape(64, 48, LANES), 6, 1, keep=())(m, kept, swapped, w_left, w_right, w_far)
    weights = lax.all_to_all(spread, "fs", 0, 0, tiled=True)

    own, common_send = call(split_body, (shape(64, 32, LANES), shape(8, 64, 8, LANES)), 1, keep=(0,))(got)
    left = shift(own, 2)
    right = shift(own, -2)
    far_a = shift(call(part_body(0), shape(32, 32, LANES), 1)(left), 2)
    far_b = shift(call(part_body(32), shape(32, 32, LANES), 1)(right), -2)
    three = call(copy_body, shape(192, 32, LANES), 3)(own, left, right)
    three = swap(three, 1)
    across = call(copy_body, shape(64, 32, LANES), 2)(far_a, far_b)
    far = swap(across, 1)

    common = lax.all_to_all(common_send, "fs", 0, 0, axis_index_groups=COLUMNS, tiled=True)
    common = call(join_body, shape(64, 48, LANES), 1)(common)

    mix_hi, mix_lo = call(mixing_body, (shape(TOK, ROWS), shape(TOK, ROWS)), 3, far=(1, 2))(pos, ids, route_weights)

    message = shape(512 + 2 * LANES, LANES)
    mine, to_right, to_left, to_far = call(
        hidden_body, (message,) * 4, 8, 1, [pltpu.VMEM((ROWS, LANES), f32)], far=(3, 4, 5, 6)
    )(m, own, left, right, across, three, far, weights)
    h_far = shift(to_far, 4)
    h_left = shift(to_right, 2)
    h_right = shift(to_left, -2)
    pair = call(pair_body, shape(4, 512 + LANES, LANES), 4)(mine, h_left, h_right, h_far)
    partner = swap(pair, 1)
    expert_out = call(down_body, shape(64, 32, LANES), 5, keep=())(mine, h_left, h_right, h_far, partner)
    returned = lax.all_to_all(expert_out, "fs", 0, 0, tiled=True)

    message = shape(64 + 2 * LANES, LANES)
    mine, to_right, to_left, to_far = call(common_hidden_body, (message,) * 4, 3, 1, far=(1,))(m, normed, common)
    c_far = shift(to_far, 4)
    c_left = shift(to_right, 2)
    c_right = shift(to_left, -2)
    pair = call(pair_body, shape(4, 64 + LANES, LANES), 4)(mine, c_left, c_right, c_far)
    partner = swap(pair, 1)
    common_out = call(common_down_body, shape(TOK, COLS, dtype=f32), 5)(mine, c_left, c_right, c_far, partner)

    serve = tuple(shape(U, D) for _ in range(3))
    gate_serve, up_serve, down_serve = call(serve_body, serve, 1, keep=())(weights)
    commons = call(serve_body, serve, 1, keep=())(common)

    mixture = call(combine_body, shape(TOK, COLS), 4, keep=())(mix_hi, mix_lo, returned, common_out)
    return (mixture, gate_serve[None], up_serve[None], down_serve[None], *commons)


def solution(mesh):
    in_specs = (
        P("fs", None),
        P("fs"),
        P("fs", "tp"),
        P("fs", "tp"),
        P("fs", "tp"),
        P("fs", "tp"),
        P("fs", "tp"),
        P("fs", "tp"),
        P("fs", None),
        P("fs", None),
    )
    out_specs = (
        P("fs", "tp"),
        P("fs", "tp", None),
        P("fs", "tp", None),
        P("fs", "tp", None),
        P("tp", None),
        P("tp", None),
        P("tp", None),
    )

    return jax.shard_map(local, mesh=mesh, in_specs=in_specs, out_specs=out_specs, check_vma=False)
```

```python
import jax
import jax.numpy as jnp
from jax import lax
from jax.experimental import pallas as pl
from jax.experimental.pallas import tpu as pltpu
from jax.sharding import PartitionSpec as P


E = 64
CAP = 16
TOP_K = 6
TOK = 128
D = 2048
N_FS = 64
N_TP = 8
U = 64
W32 = D // N_FS
COLS = D // N_TP
ROWS = E * CAP
LANES = 128
PARTS = 8
COLUMNS = [[8 * z + y for y in range(8)] for z in range(8)]
epsilon = 1e-06

f32 = jnp.float32
bf16 = jnp.bfloat16
VM = pl.BlockSpec(memory_space=pltpu.VMEM)
SM = pl.BlockSpec(memory_space=pltpu.SMEM)


def iota(shape, dim):
    return lax.broadcasted_iota(jnp.int32, shape, dim)


def half_roll(x):
    return pltpu.roll(x, 64, 1)


def call(body, outs, n_in, smem=0, scratch=(), far=(), keep=True):
    flat, tree = jax.tree.flatten(outs)
    kept = [pltpu.VMEM(o.shape, o.dtype) if keep is True or i in keep else pltpu.HBM(o.shape, o.dtype) for i, o in enumerate(flat)]
    fn = pl.pallas_call(
        body,
        out_shape=jax.tree.unflatten(tree, kept),
        in_specs=[SM] * smem + [VM] * (n_in - smem),
        out_specs=jax.tree.map(lambda _: VM, outs),
        scratch_shapes=list(scratch),
        compiler_params=pltpu.CompilerParams(vmem_limit_bytes=16 * 2**20),
    )

    def run(*args):
        placed = [
            a if i < smem else pltpu.with_memory_space_constraint(a, pltpu.HBM if i in far else pltpu.VMEM)
            for i, a in enumerate(args)
        ]
        return fn(*placed)

    return run


def dot(a, b):
    return jnp.dot(a, b, preferred_element_type=f32)


def dot_nt(a, b):
    return lax.dot_general(a, b, (((1,), (1,)), ((), ())), preferred_element_type=f32)


def gain_column(gain_ref):
    n = gain_ref.shape[1]
    eye = iota((n, n), 0) == iota((n, n), 1)
    spread = jnp.where(eye, jnp.broadcast_to(gain_ref[...], (n, n)), 0.0)
    return jnp.sum(spread, axis=1, keepdims=True)


def dispatch_body(m_ref, prompt_ref, ids_ref, gain_ref, cg_ref, cu_ref, cd_ref, send_ref, normed_ref, pos_ref):
    m = m_ref[0]
    gain = gain_column(gain_ref)
    both = jnp.concatenate([cg_ref[...] * gain, cu_ref[...] * gain], axis=1)
    down = jnp.concatenate([cd_ref[0:16, :], cd_ref[16:32, :]], axis=1)
    piece = jnp.concatenate([both, down, jnp.zeros((16, LANES), f32)], axis=0)
    parts = piece.reshape(PARTS, 8, LANES).astype(bf16)
    for z in range(N_FS // PARTS):
        send_ref[PARTS * z : PARTS * z + PARTS, 32:40, :] = parts
    values = prompt_ref[...].astype(f32)
    scale = lax.rsqrt(jnp.mean(values * values, axis=1, keepdims=True) + epsilon)
    normed_ref[...] = (values * scale).astype(bf16)
    experts = iota((E, TOK), 0)
    named = jnp.zeros((E, TOK), f32)
    for k in range(TOP_K):
        named = jnp.where(ids_ref[k : k + 1, :] == experts, 1.0, named)
    earlier = jnp.where(iota((TOK, TOK), 0) < iota((TOK, TOK), 1), 1.0, 0.0).astype(bf16)
    slot = dot(named.astype(bf16), earlier)
    pos = jnp.where(named > 0.0, slot, -1.0)
    pos_ref[...] = pos
    expand = jnp.where((iota((ROWS, E), 0) >> 4) == iota((ROWS, E), 1), 1.0, 0.0).astype(bf16)
    at = dot(expand, pos.astype(bf16))
    pick = jnp.where(at == (iota((ROWS, TOK), 0) & 15).astype(f32), 1.0, 0.0).astype(bf16)
    mine = normed_ref[:, pl.ds(pl.multiple_of(m * COLS, COLS), COLS)]
    rows = dot(pick, mine).astype(bf16)
    send_ref[:, 0:16, :] = rows[:, :LANES].reshape(E, CAP, LANES)
    send_ref[:, 16:32, :] = rows[:, LANES:].reshape(E, CAP, LANES)


def own_rows_body(got_ref, own_ref, part_ref):
    own_ref[...] = got_ref[:, 0:32, :]
    part_ref[...] = got_ref[:, 32:40, :]


def spread_body(part_ref, parts_ref):
    parts = part_ref[...]
    for y in range(PARTS):
        parts_ref[y] = parts


STEPS = (0, 2, -2, 4)


def prepare_body(m_ref, gain_ref, g_ref, u_ref, d_ref, keep_ref, swap_ref):
    m = m_ref[0]
    gain = gain_column(gain_ref)
    low = iota((W32, LANES), 1) < 64
    low16 = iota((16, LANES), 1) < 64
    for i, step in enumerate(STEPS):
        for out_ref, to in ((keep_ref, (m + step) & 7), (swap_ref, ((m + step) & 7) ^ 1)):
            odd = (to & 1) == 1
            for j in range(8):
                at = pl.ds(pl.multiple_of(j * 512 + (to >> 1) * LANES, LANES), LANES)
                g = g_ref[:, at] * gain
                u = u_ref[:, at] * gain
                d = d_ref[:, at]
                g = jnp.where(odd, half_roll(g), g)
                u = jnp.where(odd, u, half_roll(u))
                out_ref[i, j, 0:32, :] = jnp.where(low, g, u).astype(bf16)
                d0, d1 = d[0:16, :], d[16:32, :]
                d0 = jnp.where(odd, half_roll(d0), d0)
                d1 = jnp.where(odd, d1, half_roll(d1))
                out_ref[i, j, 32:48, :] = jnp.where(low16, d0, d1).astype(bf16)


def repack_body(keep_ref, swapped_ref, *out_refs):
    for i, out_ref in enumerate(out_refs):
        out_ref[0:8] = keep_ref[i]
        out_ref[8:16] = swapped_ref[i]


def assemble_body(m_ref, own_ref, left_ref, right_ref, far_ref, out_ref):
    m = m_ref[0]

    def put(t, x):
        out_ref[pl.ds(pl.multiple_of(t * 8, 8), 8)] = x

    for step, ref in zip(STEPS, (own_ref, left_ref, right_ref, far_ref)):
        t = (m - step) & 7
        put(t, ref[0:8])
        put(t ^ 1, ref[8:16])


def silu(v):
    return v / (1.0 + jnp.exp(-v))


def packed_hidden(acc):
    half = acc.shape[0] // 2
    top, bottom = acc[:half], acc[half:]
    first = silu(top) * half_roll(top)
    second = silu(half_roll(bottom)) * bottom
    return jnp.where(iota((half, LANES), 1) < 64, first, second).astype(bf16)


def copy_body(*refs):
    out_ref, at = refs[-1], 0
    for ref in refs[:-1]:
        out_ref[at : at + ref.shape[0]] = ref[...]
        at += ref.shape[0]


def part_body(at):
    def body(in_ref, out_ref):
        out_ref[...] = in_ref[at : at + out_ref.shape[0]]

    return body


def down_block(w_ref, q):
    return w_ref[pl.ds(pl.multiple_of((q & 7) * 8, 8), 8), 32:48, :].reshape(LANES, LANES)


def write_messages(m, rows, w_ref, refs):
    n = rows.shape[0]
    for ref, step in zip(refs, STEPS):
        ref[0:n, :] = rows
        ref[n : n + LANES, :] = down_block(w_ref, m + step)
        ref[n + LANES : n + 2 * LANES, :] = down_block(w_ref, (m + step) ^ 1)


def common_hidden_body(m_ref, normed_ref, parts_ref, w_ref, *to_refs):
    pieces = [parts_ref[p].astype(f32) for p in range(6)]
    w_ref[...] = jnp.concatenate(pieces, axis=1).astype(bf16)
    weights = w_ref[:, 0:32, :].reshape(D, LANES)
    write_messages(m_ref[0], packed_hidden(dot(normed_ref[...], weights)), w_ref, to_refs)


def hidden_body(m_ref, own_ref, left_ref, right_ref, across_ref, three_ref, far_ref, w_ref, *rest):
    m = m_ref[0]
    to_refs, acc_ref = rest[:4], rest[4]

    def joined(x):
        n = x.shape[0]
        return jnp.concatenate([x[:, 0:16, :].reshape(n * 16, LANES), x[:, 16:32, :].reshape(n * 16, LANES)], axis=1)

    def weights(q):
        return w_ref[pl.ds(pl.multiple_of((q & 7) * 8, 8), 8), 0:32, :].reshape(COLS, LANES)

    acc_ref[...] = dot(joined(own_ref[...]), weights(m))
    acc_ref[...] += dot(joined(left_ref[...]), weights(m - 2))
    acc_ref[...] += dot(joined(right_ref[...]), weights(m + 2))
    acc_ref[...] += dot(joined(across_ref[...]), weights(m + 4))
    other = m ^ 1
    acc_ref[...] += dot(joined(three_ref[0:64]), weights(other))
    acc_ref[...] += dot(joined(three_ref[64:128]), weights(other - 2))
    acc_ref[...] += dot(joined(three_ref[128:192]), weights(other + 2))
    acc_ref[...] += dot(joined(far_ref[...]), weights(other + 4))
    write_messages(m, packed_hidden(acc_ref[...]), w_ref, to_refs)


def pair_body(*refs):
    out_ref = refs[-1]
    n = out_ref.shape[1] - LANES
    for i, ref in enumerate(refs[:-1]):
        out_ref[i, 0:n, :] = ref[0:n, :]
        out_ref[i, n : n + LANES, :] = ref[n + LANES : n + 2 * LANES, :]


def down_parts(refs, partner_ref):
    n = partner_ref.shape[1] - LANES
    low = iota((n, LANES), 1) < 64
    low_w = iota((LANES, LANES), 1) < 64
    tops, bottoms, mats = [], [], []
    for i, ref in enumerate(refs):
        a = ref[0:n, :].astype(f32)
        b = partner_ref[i, 0:n, :].astype(f32)
        tops.append(jnp.where(low, a, half_roll(b)).astype(bf16))
        bottoms.append(jnp.where(low, half_roll(a), b).astype(bf16))
        wa = ref[n : n + LANES, :].astype(f32)
        wb = partner_ref[i, n : n + LANES, :].astype(f32)
        first = jnp.where(low_w, wa, half_roll(wb)).astype(bf16)
        second = jnp.where(low_w, half_roll(wa), wb).astype(bf16)
        parts = []
        for f in range(8):
            at = slice(16 * f, 16 * f + 16)
            parts += [first[at], second[at]]
        mats.append(jnp.concatenate(parts, axis=0))
    return tuple(jnp.concatenate(x, axis=1) for x in (tops, bottoms, mats))


def down_body(own_ref, left_ref, right_ref, far_ref, partner_ref, out_ref):
    top, bottom, mat = down_parts((own_ref, left_ref, right_ref, far_ref), partner_ref)
    for i, rows in enumerate((top, bottom)):
        r = dot_nt(rows, mat).astype(bf16)
        at = slice(32 * i, 32 * i + 32)
        out_ref[at, 0:16, :] = r[:, :LANES].reshape(32, 16, LANES)
        out_ref[at, 16:32, :] = r[:, LANES:].reshape(32, 16, LANES)


def common_down_body(own_ref, left_ref, right_ref, far_ref, partner_ref, out_ref):
    top, bottom, mat = down_parts((own_ref, left_ref, right_ref, far_ref), partner_ref)
    out_ref[0:64, :] = dot_nt(top, mat)
    out_ref[64:128, :] = dot_nt(bottom, mat)


def mixing_body(pos_ref, ids_ref, weight_ref, hi_ref, lo_ref):
    experts = iota((E, TOK), 0)
    w = jnp.zeros((E, TOK), f32)
    for k in range(TOP_K):
        w = jnp.where(ids_ref[k : k + 1, :] == experts, weight_ref[k : k + 1, :], w)
    pos = jnp.transpose(pos_ref[...]).astype(bf16)
    w = jnp.transpose(w)
    expand = jnp.where(iota((E, ROWS), 0) == (iota((E, ROWS), 1) >> 4), 1.0, 0.0).astype(bf16)
    hit = dot(pos, expand) == (iota((TOK, ROWS), 1) & 15).astype(f32)
    hi = w.astype(bf16)
    lo = (w - hi.astype(f32)).astype(bf16)
    hi_ref[...] = jnp.where(hit, dot(hi, expand), 0.0).astype(bf16)
    lo_ref[...] = jnp.where(hit, dot(lo, expand), 0.0).astype(bf16)


def combine_body(hi_ref, lo_ref, got_ref, common_ref, out_ref):
    hi, lo = hi_ref[...], lo_ref[...]
    for h in range(2):
        rows = got_ref[:, 16 * h : 16 * h + 16, :].reshape(ROWS, LANES)
        at = slice(LANES * h, LANES * h + LANES)
        out_ref[:, at] = (dot(hi, rows) + dot(lo, rows) + common_ref[:, at]).astype(bf16)


def serve_body(w_ref, g_ref, u_ref, d_ref):
    low = iota((LANES, LANES), 1) < 64
    for i in range(16):
        block = w_ref[4 * i : 4 * i + 4, 0:32, :].reshape(LANES, LANES).astype(f32)
        turned = jnp.transpose(block).astype(bf16)
        at = slice(LANES * i, LANES * i + LANES)
        g_ref[:, at] = turned[:64]
        u_ref[:, at] = turned[64:]
    for i in range(8):
        sides = []
        for s in range(2):
            straight, rolled = [], []
            for f in range(4):
                x = w_ref[8 * i + 4 * s + f, 32:48, :].astype(f32)
                y = half_roll(x)
                straight += [x, y]
                rolled += [y, x]
            sides.append(jnp.concatenate(rolled if s else straight, axis=0))
        turned = jnp.transpose(jnp.where(low, sides[0], sides[1])).astype(bf16)
        at = 256 * i
        d_ref[:, at : at + LANES] = turned[:64]
        d_ref[:, at + LANES : at + 2 * LANES] = turned[64:]


def shift(x, step):
    return lax.ppermute(x, "tp", [(i, (i + step) % N_TP) for i in range(N_TP)])


def swap(x, k):
    return lax.ppermute(x, "tp", [(i, i ^ k) for i in range(N_TP)])


def shape(*dims, dtype=bf16):
    return jax.ShapeDtypeStruct(dims, dtype)


def local(
    prompt,
    norm_gain,
    gate_train,
    up_train,
    down_train,
    common_gate_train,
    common_up_train,
    common_down_train,
    route_ids,
    route_weights,
):
    m = lax.axis_index("tp").astype(jnp.int32).reshape(1)
    ids = route_ids.T
    route_weights = route_weights.T
    gain = norm_gain.reshape(1, W32)

    send, normed, pos = call(
        dispatch_body, (shape(64, 40, LANES), shape(TOK, D), shape(E, TOK, dtype=f32)), 7, 1, far=range(8), keep=()
    )(m, prompt, ids, gain, common_gate_train, common_up_train, common_down_train)
    got = lax.all_to_all(send, "fs", 0, 0, tiled=True)

    half = shape(4, 8, 48, LANES)
    kept, to_partner = call(prepare_body, (half, half), 5, 1, far=(1,))(
        m, gain, gate_train, up_train, down_train
    )
    swapped = swap(to_partner, 1)
    message = shape(16, 48, LANES)
    w_own, to_right, to_left, to_far = call(repack_body, (message,) * 4, 2)(kept, swapped)
    w_far = shift(to_far, 4)
    w_left = shift(to_right, 2)
    w_right = shift(to_left, -2)
    spread = call(assemble_body, shape(64, 48, LANES), 5, 1, keep=())(
        m, w_own, w_left, w_right, w_far
    )
    weights = lax.all_to_all(spread, "fs", 0, 0, tiled=True)

    own, part = call(own_rows_body, (shape(64, 32, LANES), shape(64, 8, LANES)), 1, keep=(0,))(got)
    common_send = call(spread_body, shape(8, 64, 8, LANES), 1, far=(0,), keep=())(part)
    left = shift(own, 2)
    right = shift(own, -2)
    far_a = shift(call(part_body(0), shape(32, 32, LANES), 1)(left), 2)
    far_b = shift(call(part_body(32), shape(32, 32, LANES), 1)(right), -2)
    three = call(copy_body, shape(192, 32, LANES), 3)(own, left, right)
    three = swap(three, 1)
    across = call(copy_body, shape(64, 32, LANES), 2)(far_a, far_b)
    far = swap(across, 1)

    common = lax.all_to_all(common_send, "fs", 0, 0, axis_index_groups=COLUMNS, tiled=True)

    mix_hi, mix_lo = call(mixing_body, (shape(TOK, ROWS), shape(TOK, ROWS)), 3, far=(0, 1, 2), keep=())(
        pos, ids, route_weights
    )

    message = shape(512 + 2 * LANES, LANES)
    mine, to_right, to_left, to_far = call(
        hidden_body, (message,) * 4, 8, 1, [pltpu.VMEM((ROWS, LANES), f32)], far=(1, 5)
    )(m, own, left, right, across, three, far, weights)
    h_far = shift(to_far, 4)
    h_left = shift(to_right, 2)
    h_right = shift(to_left, -2)
    pair = call(pair_body, shape(4, 512 + LANES, LANES), 4)(mine, h_left, h_right, h_far)
    partner = swap(pair, 1)
    expert_out = call(down_body, shape(64, 32, LANES), 5, keep=())(mine, h_left, h_right, h_far, partner)
    returned = lax.all_to_all(expert_out, "fs", 0, 0, tiled=True)

    message = shape(64 + 2 * LANES, LANES)
    common, mine, to_right, to_left, to_far = call(
        common_hidden_body, (shape(64, 48, LANES),) + (message,) * 4, 3, 1, far=(1,)
    )(m, normed, common)
    c_far = shift(to_far, 4)
    c_left = shift(to_right, 2)
    c_right = shift(to_left, -2)
    pair = call(pair_body, shape(4, 64 + LANES, LANES), 4)(mine, c_left, c_right, c_far)
    partner = swap(pair, 1)
    common_out = call(common_down_body, shape(TOK, COLS, dtype=f32), 5)(
        mine, c_left, c_right, c_far, partner
    )

    serve = tuple(shape(U, D) for _ in range(3))
    gate_serve, up_serve, down_serve = call(serve_body, serve, 1, keep=())(weights)
    commons = call(serve_body, serve, 1, keep=())(common)

    mixture = call(combine_body, shape(TOK, COLS), 4, keep=())(mix_hi, mix_lo, returned, common_out)
    return (mixture, gate_serve[None], up_serve[None], down_serve[None], *commons)


def solution(mesh):
    in_specs = (
        P("fs", None),
        P("fs"),
        P("fs", "tp"),
        P("fs", "tp"),
        P("fs", "tp"),
        P("fs", "tp"),
        P("fs", "tp"),
        P("fs", "tp"),
        P("fs", None),
        P("fs", None),
    )
    out_specs = (
        P("fs", "tp"),
        P("fs", "tp", None),
        P("fs", "tp", None),
        P("fs", "tp", None),
        P("tp", None),
        P("tp", None),
        P("tp", None),
    )

    return jax.shard_map(local, mesh=mesh, in_specs=in_specs, out_specs=out_specs, check_vma=False)
```

```python
import jax
import jax.numpy as jnp
from jax import lax
from jax.experimental import pallas as pl
from jax.experimental.pallas import tpu as pltpu
from jax.sharding import PartitionSpec as P


E = 64
CAP = 16
TOP_K = 6
TOK = 128
D = 2048
N_FS = 64
N_TP = 8
U = 64
W32 = D // N_FS
COLS = D // N_TP
ROWS = E * CAP
LANES = 128
PARTS = 8
COLUMNS = [[8 * z + y for y in range(8)] for z in range(8)]
epsilon = 1e-06

f32 = jnp.float32
bf16 = jnp.bfloat16
VM = pl.BlockSpec(memory_space=pltpu.VMEM)
SM = pl.BlockSpec(memory_space=pltpu.SMEM)


def iota(shape, dim):
    return lax.broadcasted_iota(jnp.int32, shape, dim)


def half_roll(x):
    return pltpu.roll(x, 64, 1)


def call(body, outs, n_in, smem=0, scratch=(), far=(), keep=True):
    flat, tree = jax.tree.flatten(outs)
    kept = [pltpu.VMEM(o.shape, o.dtype) if keep is True or i in keep else pltpu.HBM(o.shape, o.dtype) for i, o in enumerate(flat)]
    fn = pl.pallas_call(
        body,
        out_shape=jax.tree.unflatten(tree, kept),
        in_specs=[SM] * smem + [VM] * (n_in - smem),
        out_specs=jax.tree.map(lambda _: VM, outs),
        scratch_shapes=list(scratch),
        compiler_params=pltpu.CompilerParams(vmem_limit_bytes=16 * 2**20),
    )

    def run(*args):
        placed = [
            a if i < smem else pltpu.with_memory_space_constraint(a, pltpu.HBM if i in far else pltpu.VMEM)
            for i, a in enumerate(args)
        ]
        return fn(*placed)

    return run


def dot(a, b):
    return jnp.dot(a, b, preferred_element_type=f32)


def dot_nt(a, b):
    return lax.dot_general(a, b, (((1,), (1,)), ((), ())), preferred_element_type=f32)


def gain_column(gain_ref):
    n = gain_ref.shape[1]
    eye = iota((n, n), 0) == iota((n, n), 1)
    spread = jnp.where(eye, jnp.broadcast_to(gain_ref[...], (n, n)), 0.0)
    return jnp.sum(spread, axis=1, keepdims=True)


def dispatch_body(m_ref, prompt_ref, ids_ref, gain_ref, cg_ref, cu_ref, cd_ref, send_ref, normed_ref, pos_ref):
    m = m_ref[0]
    gain = gain_column(gain_ref)
    both = jnp.concatenate([cg_ref[...] * gain, cu_ref[...] * gain], axis=1)
    down = jnp.concatenate([cd_ref[0:16, :], cd_ref[16:32, :]], axis=1)
    piece = jnp.concatenate([both, down, jnp.zeros((16, LANES), f32)], axis=0)
    parts = piece.reshape(PARTS, 8, LANES).astype(bf16)
    for z in range(N_FS // PARTS):
        send_ref[PARTS * z : PARTS * z + PARTS, 32:40, :] = parts
    values = prompt_ref[...].astype(f32)
    scale = lax.rsqrt(jnp.mean(values * values, axis=1, keepdims=True) + epsilon)
    normed_ref[...] = (values * scale).astype(bf16)
    experts = iota((E, TOK), 0)
    named = jnp.zeros((E, TOK), f32)
    for k in range(TOP_K):
        named = jnp.where(ids_ref[k : k + 1, :] == experts, 1.0, named)
    earlier = jnp.where(iota((TOK, TOK), 0) < iota((TOK, TOK), 1), 1.0, 0.0).astype(bf16)
    slot = dot(named.astype(bf16), earlier)
    pos = jnp.where(named > 0.0, slot, -1.0)
    pos_ref[...] = pos
    at = jnp.concatenate([jnp.broadcast_to(pos[e : e + 1, :], (CAP, TOK)) for e in range(E)], axis=0)
    pick = jnp.where(at == (iota((ROWS, TOK), 0) & 15).astype(f32), 1.0, 0.0).astype(bf16)
    mine = normed_ref[:, pl.ds(pl.multiple_of(m * COLS, COLS), COLS)]
    rows = dot(pick, mine).astype(bf16)
    send_ref[:, 0:16, :] = rows[:, :LANES].reshape(E, CAP, LANES)
    send_ref[:, 16:32, :] = rows[:, LANES:].reshape(E, CAP, LANES)


def own_rows_body(got_ref, own_ref, part_ref):
    own_ref[...] = got_ref[:, 0:32, :]
    part_ref[...] = got_ref[:, 32:40, :]


def spread_body(part_ref, parts_ref):
    parts = part_ref[...]
    for y in range(PARTS):
        parts_ref[y] = parts


STEPS = (0, 2, -2, 4)


def prepare_body(m_ref, gain_ref, g_ref, u_ref, d_ref, keep_ref, swap_ref):
    m = m_ref[0]
    gain = gain_column(gain_ref)
    low = iota((W32, LANES), 1) < 64
    low16 = iota((16, LANES), 1) < 64
    for i, step in enumerate(STEPS):
        for out_ref, to in ((keep_ref, (m + step) & 7), (swap_ref, ((m + step) & 7) ^ 1)):
            odd = (to & 1) == 1
            for j in range(8):
                at = pl.ds(pl.multiple_of(j * 512 + (to >> 1) * LANES, LANES), LANES)
                g = g_ref[:, at] * gain
                u = u_ref[:, at] * gain
                d = d_ref[:, at]
                g = jnp.where(odd, half_roll(g), g)
                u = jnp.where(odd, u, half_roll(u))
                out_ref[i, j, 0:32, :] = jnp.where(low, g, u).astype(bf16)
                d0, d1 = d[0:16, :], d[16:32, :]
                d0 = jnp.where(odd, half_roll(d0), d0)
                d1 = jnp.where(odd, d1, half_roll(d1))
                out_ref[i, j, 32:48, :] = jnp.where(low16, d0, d1).astype(bf16)


def repack_body(keep_ref, swapped_ref, *out_refs):
    for i, out_ref in enumerate(out_refs):
        out_ref[0:8] = keep_ref[i]
        out_ref[8:16] = swapped_ref[i]


def assemble_body(m_ref, own_ref, left_ref, right_ref, far_ref, out_ref):
    m = m_ref[0]

    def put(t, x):
        out_ref[pl.ds(pl.multiple_of(t * 8, 8), 8)] = x

    for step, ref in zip(STEPS, (own_ref, left_ref, right_ref, far_ref)):
        t = (m - step) & 7
        put(t, ref[0:8])
        put(t ^ 1, ref[8:16])


def silu(v):
    return v / (1.0 + jnp.exp(-v))


def packed_hidden(acc):
    half = acc.shape[0] // 2
    top, bottom = acc[:half], acc[half:]
    first = silu(top) * half_roll(top)
    second = silu(half_roll(bottom)) * bottom
    return jnp.where(iota((half, LANES), 1) < 64, first, second).astype(bf16)


def copy_body(*refs):
    out_ref, at = refs[-1], 0
    for ref in refs[:-1]:
        out_ref[at : at + ref.shape[0]] = ref[...]
        at += ref.shape[0]


def part_body(at):
    def body(in_ref, out_ref):
        out_ref[...] = in_ref[at : at + out_ref.shape[0]]

    return body


def down_block(w_ref, q):
    return w_ref[pl.ds(pl.multiple_of((q & 7) * 8, 8), 8), 32:48, :].reshape(LANES, LANES)


def write_messages(m, rows, w_ref, refs):
    n = rows.shape[0]
    for ref, step in zip(refs, STEPS):
        ref[0:n, :] = rows
        ref[n : n + LANES, :] = down_block(w_ref, m + step)
        ref[n + LANES : n + 2 * LANES, :] = down_block(w_ref, (m + step) ^ 1)


def common_hidden_body(m_ref, normed_ref, parts_ref, w_ref, *to_refs):
    pieces = [parts_ref[p].astype(f32) for p in range(6)]
    w_ref[...] = jnp.concatenate(pieces, axis=1).astype(bf16)
    weights = w_ref[:, 0:32, :].reshape(D, LANES)
    write_messages(m_ref[0], packed_hidden(dot(normed_ref[...], weights)), w_ref, to_refs)


def hidden_body(m_ref, own_ref, left_ref, right_ref, across_ref, three_ref, far_ref, w_ref, *rest):
    m = m_ref[0]
    to_refs, acc_ref = rest[:4], rest[4]

    def joined(x):
        n = x.shape[0]
        return jnp.concatenate([x[:, 0:16, :].reshape(n * 16, LANES), x[:, 16:32, :].reshape(n * 16, LANES)], axis=1)

    def weights(q):
        return w_ref[pl.ds(pl.multiple_of((q & 7) * 8, 8), 8), 0:32, :].reshape(COLS, LANES)

    acc_ref[...] = dot(joined(own_ref[...]), weights(m))
    acc_ref[...] += dot(joined(left_ref[...]), weights(m - 2))
    acc_ref[...] += dot(joined(right_ref[...]), weights(m + 2))
    acc_ref[...] += dot(joined(across_ref[...]), weights(m + 4))
    other = m ^ 1
    acc_ref[...] += dot(joined(three_ref[0:64]), weights(other))
    acc_ref[...] += dot(joined(three_ref[64:128]), weights(other - 2))
    acc_ref[...] += dot(joined(three_ref[128:192]), weights(other + 2))
    acc_ref[...] += dot(joined(far_ref[...]), weights(other + 4))
    write_messages(m, packed_hidden(acc_ref[...]), w_ref, to_refs)


def pair_body(*refs):
    out_ref = refs[-1]
    n = out_ref.shape[1] - LANES
    for i, ref in enumerate(refs[:-1]):
        out_ref[i, 0:n, :] = ref[0:n, :]
        out_ref[i, n : n + LANES, :] = ref[n + LANES : n + 2 * LANES, :]


def down_parts(refs, partner_ref):
    n = partner_ref.shape[1] - LANES
    low = iota((n, LANES), 1) < 64
    low_w = iota((LANES, LANES), 1) < 64
    tops, bottoms, mats = [], [], []
    for i, ref in enumerate(refs):
        a = ref[0:n, :].astype(f32)
        b = partner_ref[i, 0:n, :].astype(f32)
        tops.append(jnp.where(low, a, half_roll(b)).astype(bf16))
        bottoms.append(jnp.where(low, half_roll(a), b).astype(bf16))
        wa = ref[n : n + LANES, :].astype(f32)
        wb = partner_ref[i, n : n + LANES, :].astype(f32)
        first = jnp.where(low_w, wa, half_roll(wb)).astype(bf16)
        second = jnp.where(low_w, half_roll(wa), wb).astype(bf16)
        parts = []
        for f in range(8):
            at = slice(16 * f, 16 * f + 16)
            parts += [first[at], second[at]]
        mats.append(jnp.concatenate(parts, axis=0))
    return tuple(jnp.concatenate(x, axis=1) for x in (tops, bottoms, mats))


def down_body(own_ref, left_ref, right_ref, far_ref, partner_ref, out_ref):
    top, bottom, mat = down_parts((own_ref, left_ref, right_ref, far_ref), partner_ref)
    for i, rows in enumerate((top, bottom)):
        r = dot_nt(rows, mat).astype(bf16)
        at = slice(32 * i, 32 * i + 32)
        out_ref[at, 0:16, :] = r[:, :LANES].reshape(32, 16, LANES)
        out_ref[at, 16:32, :] = r[:, LANES:].reshape(32, 16, LANES)


def common_down_body(own_ref, left_ref, right_ref, far_ref, partner_ref, out_ref):
    top, bottom, mat = down_parts((own_ref, left_ref, right_ref, far_ref), partner_ref)
    out_ref[0:64, :] = dot_nt(top, mat)
    out_ref[64:128, :] = dot_nt(bottom, mat)


def mixing_body(pos_ref, ids_ref, weight_ref, hi_ref, lo_ref):
    experts = iota((E, TOK), 0)
    w = jnp.zeros((E, TOK), f32)
    for k in range(TOP_K):
        w = jnp.where(ids_ref[k : k + 1, :] == experts, weight_ref[k : k + 1, :], w)
    pos = jnp.transpose(pos_ref[...]).astype(bf16)
    w = jnp.transpose(w)
    expand = jnp.where(iota((E, ROWS), 0) == (iota((E, ROWS), 1) >> 4), 1.0, 0.0).astype(bf16)
    hit = dot(pos, expand) == (iota((TOK, ROWS), 1) & 15).astype(f32)
    hi = w.astype(bf16)
    lo = (w - hi.astype(f32)).astype(bf16)
    hi_ref[...] = jnp.where(hit, dot(hi, expand), 0.0).astype(bf16)
    lo_ref[...] = jnp.where(hit, dot(lo, expand), 0.0).astype(bf16)


def combine_body(hi_ref, lo_ref, got_ref, common_ref, out_ref):
    hi, lo = hi_ref[...], lo_ref[...]
    for h in range(2):
        rows = got_ref[:, 16 * h : 16 * h + 16, :].reshape(ROWS, LANES)
        at = slice(LANES * h, LANES * h + LANES)
        out_ref[:, at] = (dot(hi, rows) + dot(lo, rows) + common_ref[:, at]).astype(bf16)


def serve_body(w_ref, g_ref, u_ref, d_ref):
    low = iota((LANES, LANES), 1) < 64
    for i in range(16):
        block = w_ref[4 * i : 4 * i + 4, 0:32, :].reshape(LANES, LANES).astype(f32)
        turned = jnp.transpose(block).astype(bf16)
        at = slice(LANES * i, LANES * i + LANES)
        g_ref[:, at] = turned[:64]
        u_ref[:, at] = turned[64:]
    for i in range(8):
        sides = []
        for s in range(2):
            straight, rolled = [], []
            for f in range(4):
                x = w_ref[8 * i + 4 * s + f, 32:48, :].astype(f32)
                y = half_roll(x)
                straight += [x, y]
                rolled += [y, x]
            sides.append(jnp.concatenate(rolled if s else straight, axis=0))
        turned = jnp.transpose(jnp.where(low, sides[0], sides[1])).astype(bf16)
        at = 256 * i
        d_ref[:, at : at + LANES] = turned[:64]
        d_ref[:, at + LANES : at + 2 * LANES] = turned[64:]


def shift(x, step):
    return lax.ppermute(x, "tp", [(i, (i + step) % N_TP) for i in range(N_TP)])


def swap(x, k):
    return lax.ppermute(x, "tp", [(i, i ^ k) for i in range(N_TP)])


def shape(*dims, dtype=bf16):
    return jax.ShapeDtypeStruct(dims, dtype)


def local(
    prompt,
    norm_gain,
    gate_train,
    up_train,
    down_train,
    common_gate_train,
    common_up_train,
    common_down_train,
    route_ids,
    route_weights,
):
    m = lax.axis_index("tp").astype(jnp.int32).reshape(1)
    ids = route_ids.T
    route_weights = route_weights.T
    gain = norm_gain.reshape(1, W32)

    send, normed, pos = call(
        dispatch_body, (shape(64, 40, LANES), shape(TOK, D), shape(E, TOK, dtype=f32)), 7, 1, far=range(8), keep=()
    )(m, prompt, ids, gain, common_gate_train, common_up_train, common_down_train)
    got = lax.all_to_all(send, "fs", 0, 0, tiled=True)

    half = shape(4, 8, 48, LANES)
    kept, to_partner = call(prepare_body, (half, half), 5, 1, far=(1,))(
        m, gain, gate_train, up_train, down_train
    )
    swapped = swap(to_partner, 1)
    message = shape(16, 48, LANES)
    w_own, to_right, to_left, to_far = call(repack_body, (message,) * 4, 2)(kept, swapped)
    w_far = shift(to_far, 4)
    w_left = shift(to_right, 2)
    w_right = shift(to_left, -2)
    spread = call(assemble_body, shape(64, 48, LANES), 5, 1, keep=())(
        m, w_own, w_left, w_right, w_far
    )
    weights = lax.all_to_all(spread, "fs", 0, 0, tiled=True)

    own, part = call(own_rows_body, (shape(64, 32, LANES), shape(64, 8, LANES)), 1, keep=(0,))(got)
    common_send = call(spread_body, shape(8, 64, 8, LANES), 1, far=(0,), keep=())(part)
    left = shift(own, 2)
    right = shift(own, -2)
    far_a = shift(call(part_body(0), shape(32, 32, LANES), 1)(left), 2)
    far_b = shift(call(part_body(32), shape(32, 32, LANES), 1)(right), -2)
    three = call(copy_body, shape(192, 32, LANES), 3)(own, left, right)
    three = swap(three, 1)
    across = call(copy_body, shape(64, 32, LANES), 2)(far_a, far_b)
    far = swap(across, 1)

    common = lax.all_to_all(common_send, "fs", 0, 0, axis_index_groups=COLUMNS, tiled=True)

    mix_hi, mix_lo = call(mixing_body, (shape(TOK, ROWS), shape(TOK, ROWS)), 3, far=(0, 1, 2), keep=())(
        pos, ids, route_weights
    )

    message = shape(512 + 2 * LANES, LANES)
    mine, to_right, to_left, to_far = call(
        hidden_body, (message,) * 4, 8, 1, [pltpu.VMEM((ROWS, LANES), f32)], far=(1, 5)
    )(m, own, left, right, across, three, far, weights)
    h_far = shift(to_far, 4)
    h_left = shift(to_right, 2)
    h_right = shift(to_left, -2)
    pair = call(pair_body, shape(4, 512 + LANES, LANES), 4)(mine, h_left, h_right, h_far)
    partner = swap(pair, 1)
    expert_out = call(down_body, shape(64, 32, LANES), 5, keep=())(mine, h_left, h_right, h_far, partner)
    returned = lax.all_to_all(expert_out, "fs", 0, 0, tiled=True)

    message = shape(64 + 2 * LANES, LANES)
    common, mine, to_right, to_left, to_far = call(
        common_hidden_body, (shape(64, 48, LANES),) + (message,) * 4, 3, 1
    )(m, normed, common)
    c_far = shift(to_far, 4)
    c_left = shift(to_right, 2)
    c_right = shift(to_left, -2)
    pair = call(pair_body, shape(4, 64 + LANES, LANES), 4)(mine, c_left, c_right, c_far)
    partner = swap(pair, 1)
    common_out = call(common_down_body, shape(TOK, COLS, dtype=f32), 5)(
        mine, c_left, c_right, c_far, partner
    )

    serve = tuple(shape(U, D) for _ in range(3))
    gate_serve, up_serve, down_serve = call(serve_body, serve, 1, keep=())(weights)
    commons = call(serve_body, serve, 1, keep=())(common)

    mixture = call(combine_body, shape(TOK, COLS), 4, keep=())(mix_hi, mix_lo, returned, common_out)
    return (mixture, gate_serve[None], up_serve[None], down_serve[None], *commons)


def solution(mesh):
    in_specs = (
        P("fs", None),
        P("fs"),
        P("fs", "tp"),
        P("fs", "tp"),
        P("fs", "tp"),
        P("fs", "tp"),
        P("fs", "tp"),
        P("fs", "tp"),
        P("fs", None),
        P("fs", None),
    )
    out_specs = (
        P("fs", "tp"),
        P("fs", "tp", None),
        P("fs", "tp", None),
        P("fs", "tp", None),
        P("tp", None),
        P("tp", None),
        P("tp", None),
    )

    return jax.shard_map(local, mesh=mesh, in_specs=in_specs, out_specs=out_specs, check_vma=False)
```

```python
import jax
import jax.numpy as jnp
from jax import lax
from jax.experimental import pallas as pl
from jax.experimental.pallas import tpu as pltpu
from jax.sharding import PartitionSpec as P


E = 64
CAP = 16
TOP_K = 6
TOK = 128
D = 2048
N_FS = 64
N_TP = 8
U = 64
W32 = D // N_FS
COLS = D // N_TP
ROWS = E * CAP
LANES = 128
PARTS = 8
COLUMNS = [[8 * z + y for y in range(8)] for z in range(8)]
epsilon = 1e-06

f32 = jnp.float32
bf16 = jnp.bfloat16
VM = pl.BlockSpec(memory_space=pltpu.VMEM)
SM = pl.BlockSpec(memory_space=pltpu.SMEM)


def iota(shape, dim):
    return lax.broadcasted_iota(jnp.int32, shape, dim)


def half_roll(x):
    return pltpu.roll(x, 64, 1)


def call(body, outs, n_in, smem=0, scratch=(), far=(), keep=True):
    flat, tree = jax.tree.flatten(outs)
    kept = [pltpu.VMEM(o.shape, o.dtype) if keep is True or i in keep else pltpu.HBM(o.shape, o.dtype) for i, o in enumerate(flat)]
    fn = pl.pallas_call(
        body,
        out_shape=jax.tree.unflatten(tree, kept),
        in_specs=[SM] * smem + [VM] * (n_in - smem),
        out_specs=jax.tree.map(lambda _: VM, outs),
        scratch_shapes=list(scratch),
        compiler_params=pltpu.CompilerParams(vmem_limit_bytes=16 * 2**20),
    )

    def run(*args):
        placed = [
            a if i < smem else pltpu.with_memory_space_constraint(a, pltpu.HBM if i in far else pltpu.VMEM)
            for i, a in enumerate(args)
        ]
        return fn(*placed)

    return run


def dot(a, b):
    return jnp.dot(a, b, preferred_element_type=f32)


def dot_nt(a, b):
    return lax.dot_general(a, b, (((1,), (1,)), ((), ())), preferred_element_type=f32)


def gain_column(gain_ref):
    n = gain_ref.shape[1]
    eye = iota((n, n), 0) == iota((n, n), 1)
    spread = jnp.where(eye, jnp.broadcast_to(gain_ref[...], (n, n)), 0.0)
    return jnp.sum(spread, axis=1, keepdims=True)


def dispatch_body(m_ref, prompt_ref, ids_ref, gain_ref, cg_ref, cu_ref, cd_ref, send_ref, normed_ref, pos_ref):
    m = m_ref[0]
    gain = gain_column(gain_ref)
    both = jnp.concatenate([cg_ref[...] * gain, cu_ref[...] * gain], axis=1)
    down = jnp.concatenate([cd_ref[0:16, :], cd_ref[16:32, :]], axis=1)
    piece = jnp.concatenate([both, down, jnp.zeros((16, LANES), f32)], axis=0)
    parts = piece.reshape(PARTS, 8, LANES).astype(bf16)
    for z in range(N_FS // PARTS):
        send_ref[PARTS * z : PARTS * z + PARTS, 32:40, :] = parts
    values = prompt_ref[...].astype(f32)
    scale = lax.rsqrt(jnp.mean(values * values, axis=1, keepdims=True) + epsilon)
    normed_ref[...] = (values * scale).astype(bf16)
    experts = iota((E, TOK), 0)
    named = jnp.zeros((E, TOK), f32)
    for k in range(TOP_K):
        named = jnp.where(ids_ref[k : k + 1, :] == experts, 1.0, named)
    earlier = jnp.where(iota((TOK, TOK), 0) < iota((TOK, TOK), 1), 1.0, 0.0).astype(bf16)
    slot = dot(named.astype(bf16), earlier)
    pos = jnp.where(named > 0.0, slot, -1.0)
    pos_ref[...] = pos
    at = jnp.concatenate([jnp.broadcast_to(pos[e : e + 1, :], (CAP, TOK)) for e in range(E)], axis=0)
    pick = jnp.where(at == (iota((ROWS, TOK), 0) & 15).astype(f32), 1.0, 0.0).astype(bf16)
    mine = normed_ref[:, pl.ds(pl.multiple_of(m * COLS, COLS), COLS)]
    rows = dot(pick, mine).astype(bf16)
    send_ref[:, 0:16, :] = rows[:, :LANES].reshape(E, CAP, LANES)
    send_ref[:, 16:32, :] = rows[:, LANES:].reshape(E, CAP, LANES)


def own_rows_body(got_ref, own_ref):
    own_ref[...] = got_ref[:, 0:32, :]


def spread_body(got_ref, parts_ref):
    parts = got_ref[:, 32:40, :]
    for y in range(PARTS):
        parts_ref[y] = parts


STEPS = (0, 2, -2, 4)


def prepare_body(m_ref, gain_ref, g_ref, u_ref, d_ref, keep_ref, swap_ref):
    m = m_ref[0]
    gain = gain_column(gain_ref)
    low = iota((W32, LANES), 1) < 64
    low16 = iota((16, LANES), 1) < 64
    for i, step in enumerate(STEPS):
        for out_ref, to in ((keep_ref, (m + step) & 7), (swap_ref, ((m + step) & 7) ^ 1)):
            odd = (to & 1) == 1
            for j in range(8):
                at = pl.ds(pl.multiple_of(j * 512 + (to >> 1) * LANES, LANES), LANES)
                g = g_ref[:, at] * gain
                u = u_ref[:, at] * gain
                d = d_ref[:, at]
                g = jnp.where(odd, half_roll(g), g)
                u = jnp.where(odd, u, half_roll(u))
                out_ref[i, j, 0:32, :] = jnp.where(low, g, u).astype(bf16)
                d0, d1 = d[0:16, :], d[16:32, :]
                d0 = jnp.where(odd, half_roll(d0), d0)
                d1 = jnp.where(odd, d1, half_roll(d1))
                out_ref[i, j, 32:48, :] = jnp.where(low16, d0, d1).astype(bf16)


def repack_body(keep_ref, swapped_ref, *out_refs):
    for i, out_ref in enumerate(out_refs):
        out_ref[0:8] = keep_ref[i]
        out_ref[8:16] = swapped_ref[i]


def assemble_body(m_ref, own_ref, left_ref, right_ref, far_ref, out_ref):
    m = m_ref[0]

    def put(t, x):
        out_ref[pl.ds(pl.multiple_of(t * 8, 8), 8)] = x

    for step, ref in zip(STEPS, (own_ref, left_ref, right_ref, far_ref)):
        t = (m - step) & 7
        put(t, ref[0:8])
        put(t ^ 1, ref[8:16])


def silu(v):
    return v / (1.0 + jnp.exp(-v))


def packed_hidden(acc):
    half = acc.shape[0] // 2
    top, bottom = acc[:half], acc[half:]
    first = silu(top) * half_roll(top)
    second = silu(half_roll(bottom)) * bottom
    return jnp.where(iota((half, LANES), 1) < 64, first, second).astype(bf16)


def copy_body(*refs):
    out_ref, at = refs[-1], 0
    for ref in refs[:-1]:
        out_ref[at : at + ref.shape[0]] = ref[...]
        at += ref.shape[0]


def part_body(at):
    def body(in_ref, out_ref):
        out_ref[...] = in_ref[at : at + out_ref.shape[0]]

    return body


def down_block(w_ref, q):
    return w_ref[pl.ds(pl.multiple_of((q & 7) * 8, 8), 8), 32:48, :].reshape(LANES, LANES)


def write_messages(m, rows, w_ref, refs):
    n = rows.shape[0]
    for ref, step in zip(refs, STEPS):
        ref[0:n, :] = rows
        ref[n : n + LANES, :] = down_block(w_ref, m + step)
        ref[n + LANES : n + 2 * LANES, :] = down_block(w_ref, (m + step) ^ 1)


def common_hidden_body(m_ref, normed_ref, parts_ref, w_ref, *to_refs):
    pieces = [parts_ref[p].astype(f32) for p in range(6)]
    w_ref[...] = jnp.concatenate(pieces, axis=1).astype(bf16)
    weights = w_ref[:, 0:32, :].reshape(D, LANES)
    write_messages(m_ref[0], packed_hidden(dot(normed_ref[...], weights)), w_ref, to_refs)


def hidden_body(m_ref, own_ref, left_ref, right_ref, across_ref, three_ref, far_ref, w_ref, *rest):
    m = m_ref[0]
    to_refs, acc_ref = rest[:4], rest[4]

    def joined(x):
        n = x.shape[0]
        return jnp.concatenate([x[:, 0:16, :].reshape(n * 16, LANES), x[:, 16:32, :].reshape(n * 16, LANES)], axis=1)

    def weights(q):
        return w_ref[pl.ds(pl.multiple_of((q & 7) * 8, 8), 8), 0:32, :].reshape(COLS, LANES)

    acc_ref[...] = dot(joined(own_ref[...]), weights(m))
    acc_ref[...] += dot(joined(left_ref[...]), weights(m - 2))
    acc_ref[...] += dot(joined(right_ref[...]), weights(m + 2))
    acc_ref[...] += dot(joined(across_ref[...]), weights(m + 4))
    other = m ^ 1
    acc_ref[...] += dot(joined(three_ref[0:64]), weights(other))
    acc_ref[...] += dot(joined(three_ref[64:128]), weights(other - 2))
    acc_ref[...] += dot(joined(three_ref[128:192]), weights(other + 2))
    acc_ref[...] += dot(joined(far_ref[...]), weights(other + 4))
    write_messages(m, packed_hidden(acc_ref[...]), w_ref, to_refs)


def pair_body(*refs):
    out_ref = refs[-1]
    n = out_ref.shape[1] - LANES
    for i, ref in enumerate(refs[:-1]):
        out_ref[i, 0:n, :] = ref[0:n, :]
        out_ref[i, n : n + LANES, :] = ref[n + LANES : n + 2 * LANES, :]


def down_parts(refs, partner_ref):
    n = partner_ref.shape[1] - LANES
    low = iota((n, LANES), 1) < 64
    low_w = iota((LANES, LANES), 1) < 64
    tops, bottoms, mats = [], [], []
    for i, ref in enumerate(refs):
        a = ref[0:n, :].astype(f32)
        b = partner_ref[i, 0:n, :].astype(f32)
        tops.append(jnp.where(low, a, half_roll(b)).astype(bf16))
        bottoms.append(jnp.where(low, half_roll(a), b).astype(bf16))
        wa = ref[n : n + LANES, :].astype(f32)
        wb = partner_ref[i, n : n + LANES, :].astype(f32)
        first = jnp.where(low_w, wa, half_roll(wb)).astype(bf16)
        second = jnp.where(low_w, half_roll(wa), wb).astype(bf16)
        parts = []
        for f in range(8):
            at = slice(16 * f, 16 * f + 16)
            parts += [first[at], second[at]]
        mats.append(jnp.concatenate(parts, axis=0))
    return tuple(jnp.concatenate(x, axis=1) for x in (tops, bottoms, mats))


def down_body(own_ref, left_ref, right_ref, far_ref, partner_ref, out_ref):
    top, bottom, mat = down_parts((own_ref, left_ref, right_ref, far_ref), partner_ref)
    for i, rows in enumerate((top, bottom)):
        r = dot_nt(rows, mat).astype(bf16)
        at = slice(32 * i, 32 * i + 32)
        out_ref[at, 0:16, :] = r[:, :LANES].reshape(32, 16, LANES)
        out_ref[at, 16:32, :] = r[:, LANES:].reshape(32, 16, LANES)


def common_down_body(own_ref, left_ref, right_ref, far_ref, partner_ref, out_ref):
    top, bottom, mat = down_parts((own_ref, left_ref, right_ref, far_ref), partner_ref)
    out_ref[0:64, :] = dot_nt(top, mat)
    out_ref[64:128, :] = dot_nt(bottom, mat)


def mixing_body(pos_ref, ids_ref, weight_ref, hi_ref, lo_ref):
    experts = iota((E, TOK), 0)
    w = jnp.zeros((E, TOK), f32)
    for k in range(TOP_K):
        w = jnp.where(ids_ref[k : k + 1, :] == experts, weight_ref[k : k + 1, :], w)
    pos = jnp.transpose(pos_ref[...]).astype(bf16)
    w = jnp.transpose(w)
    expand = jnp.where(iota((E, ROWS), 0) == (iota((E, ROWS), 1) >> 4), 1.0, 0.0).astype(bf16)
    hit = dot(pos, expand) == (iota((TOK, ROWS), 1) & 15).astype(f32)
    hi = w.astype(bf16)
    lo = (w - hi.astype(f32)).astype(bf16)
    hi_ref[...] = jnp.where(hit, dot(hi, expand), 0.0).astype(bf16)
    lo_ref[...] = jnp.where(hit, dot(lo, expand), 0.0).astype(bf16)


def combine_body(hi_ref, lo_ref, got_ref, common_ref, out_ref):
    hi, lo = hi_ref[...], lo_ref[...]
    for h in range(2):
        rows = got_ref[:, 16 * h : 16 * h + 16, :].reshape(ROWS, LANES)
        at = slice(LANES * h, LANES * h + LANES)
        out_ref[:, at] = (dot(hi, rows) + dot(lo, rows) + common_ref[:, at]).astype(bf16)


def serve_body(w_ref, g_ref, u_ref, d_ref):
    low = iota((LANES, LANES), 1) < 64
    for i in range(16):
        block = w_ref[4 * i : 4 * i + 4, 0:32, :].reshape(LANES, LANES).astype(f32)
        turned = jnp.transpose(block).astype(bf16)
        at = slice(LANES * i, LANES * i + LANES)
        g_ref[:, at] = turned[:64]
        u_ref[:, at] = turned[64:]
    for i in range(8):
        sides = []
        for s in range(2):
            straight, rolled = [], []
            for f in range(4):
                x = w_ref[8 * i + 4 * s + f, 32:48, :].astype(f32)
                y = half_roll(x)
                straight += [x, y]
                rolled += [y, x]
            sides.append(jnp.concatenate(rolled if s else straight, axis=0))
        turned = jnp.transpose(jnp.where(low, sides[0], sides[1])).astype(bf16)
        at = 256 * i
        d_ref[:, at : at + LANES] = turned[:64]
        d_ref[:, at + LANES : at + 2 * LANES] = turned[64:]


def shift(x, step):
    return lax.ppermute(x, "tp", [(i, (i + step) % N_TP) for i in range(N_TP)])


def swap(x, k):
    return lax.ppermute(x, "tp", [(i, i ^ k) for i in range(N_TP)])


def shape(*dims, dtype=bf16):
    return jax.ShapeDtypeStruct(dims, dtype)


def local(
    prompt,
    norm_gain,
    gate_train,
    up_train,
    down_train,
    common_gate_train,
    common_up_train,
    common_down_train,
    route_ids,
    route_weights,
):
    m = lax.axis_index("tp").astype(jnp.int32).reshape(1)
    ids = route_ids.T
    route_weights = route_weights.T
    gain = norm_gain.reshape(1, W32)

    send, normed, pos = call(
        dispatch_body, (shape(64, 40, LANES), shape(TOK, D), shape(E, TOK, dtype=f32)), 7, 1, far=range(8), keep=()
    )(m, prompt, ids, gain, common_gate_train, common_up_train, common_down_train)
    got = lax.all_to_all(send, "fs", 0, 0, tiled=True)

    half = shape(4, 8, 48, LANES)
    kept, to_partner = call(prepare_body, (half, half), 5, 1, far=(1,))(
        m, gain, gate_train, up_train, down_train
    )
    swapped = swap(to_partner, 1)
    message = shape(16, 48, LANES)
    w_own, to_right, to_left, to_far = call(repack_body, (message,) * 4, 2)(kept, swapped)
    w_far = shift(to_far, 4)
    w_left = shift(to_right, 2)
    w_right = shift(to_left, -2)
    spread = call(assemble_body, shape(64, 48, LANES), 5, 1, keep=())(
        m, w_own, w_left, w_right, w_far
    )
    weights = lax.all_to_all(spread, "fs", 0, 0, tiled=True)

    own = call(own_rows_body, shape(64, 32, LANES), 1)(got)
    common_send = call(spread_body, shape(8, 64, 8, LANES), 1, keep=())(got)
    left = shift(own, 2)
    right = shift(own, -2)
    far_a = shift(call(part_body(0), shape(32, 32, LANES), 1)(left), 2)
    far_b = shift(call(part_body(32), shape(32, 32, LANES), 1)(right), -2)
    three = call(copy_body, shape(192, 32, LANES), 3)(own, left, right)
    three = swap(three, 1)
    across = call(copy_body, shape(64, 32, LANES), 2)(far_a, far_b)
    far = swap(across, 1)

    common = lax.all_to_all(common_send, "fs", 0, 0, axis_index_groups=COLUMNS, tiled=True)

    mix_hi, mix_lo = call(mixing_body, (shape(TOK, ROWS), shape(TOK, ROWS)), 3, far=(0, 1, 2), keep=())(
        pos, ids, route_weights
    )

    message = shape(512 + 2 * LANES, LANES)
    mine, to_right, to_left, to_far = call(
        hidden_body, (message,) * 4, 8, 1, [pltpu.VMEM((ROWS, LANES), f32)], far=(1, 5)
    )(m, own, left, right, across, three, far, weights)
    h_far = shift(to_far, 4)
    h_left = shift(to_right, 2)
    h_right = shift(to_left, -2)
    pair = call(pair_body, shape(4, 512 + LANES, LANES), 4)(mine, h_left, h_right, h_far)
    partner = swap(pair, 1)
    expert_out = call(down_body, shape(64, 32, LANES), 5, keep=())(mine, h_left, h_right, h_far, partner)
    returned = lax.all_to_all(expert_out, "fs", 0, 0, tiled=True)

    message = shape(64 + 2 * LANES, LANES)
    common, mine, to_right, to_left, to_far = call(
        common_hidden_body, (shape(64, 48, LANES),) + (message,) * 4, 3, 1
    )(m, normed, common)
    c_far = shift(to_far, 4)
    c_left = shift(to_right, 2)
    c_right = shift(to_left, -2)
    pair = call(pair_body, shape(4, 64 + LANES, LANES), 4)(mine, c_left, c_right, c_far)
    partner = swap(pair, 1)
    common_out = call(common_down_body, shape(TOK, COLS, dtype=f32), 5)(
        mine, c_left, c_right, c_far, partner
    )

    serve = tuple(shape(U, D) for _ in range(3))
    gate_serve, up_serve, down_serve = call(serve_body, serve, 1, keep=())(weights)
    commons = call(serve_body, serve, 1, keep=())(common)

    mixture = call(combine_body, shape(TOK, COLS), 4, keep=())(mix_hi, mix_lo, returned, common_out)
    return (mixture, gate_serve[None], up_serve[None], down_serve[None], *commons)


def solution(mesh):
    in_specs = (
        P("fs", None),
        P("fs"),
        P("fs", "tp"),
        P("fs", "tp"),
        P("fs", "tp"),
        P("fs", "tp"),
        P("fs", "tp"),
        P("fs", "tp"),
        P("fs", None),
        P("fs", None),
    )
    out_specs = (
        P("fs", "tp"),
        P("fs", "tp", None),
        P("fs", "tp", None),
        P("fs", "tp", None),
        P("tp", None),
        P("tp", None),
        P("tp", None),
    )

    return jax.shard_map(local, mesh=mesh, in_specs=in_specs, out_specs=out_specs, check_vma=False)
```
